32 devices in a mesh: sp: 8 (over z, x), tp: 4 (over y, core).
Axes of the slice: x: 2, y: 2, z: 4, core: 2. Of those that a mesh axis runs over, the one named last changes fastest.
Arguments:
- tokens: bfloat16 [2048, 2048], P('sp'), may hold values from -6 to 6
- documents: int32 [2048], P('sp'), may hold values from 0 to 3, never falling along the last dimension, each value on 1 to 1024 neighbouring positions
- norm_gain: float32 [1, 2048], replicated, may hold values from 0.1 to 1.9
- w_query: bfloat16 [1, 2048, 2048], P(None, 'sp', 'tp'), may hold values from -0.125 to 0.125
- w_key: bfloat16 [1, 2048, 2048], P(None, 'sp', 'tp'), may hold values from -0.125 to 0.125
- w_value: bfloat16 [1, 2048, 2048], P(None, 'sp', 'tp'), may hold values from -0.125 to 0.125
- w_out: bfloat16 [1, 2048, 2048], P(None, None, 'sp'), may hold values from -0.59765625 to 0.59765625
- rel_bias: float32 [1, 32, 257], P(None, 'tp'), may hold values from -8 to 240
Outputs:
- mixed: bfloat16 [2048, 2048], P('sp')
The draws below stay inside these ranges and needn't reach their ends.
Inputs may be any that keep to these rules, and one draw needn't show every extreme that they name: `documents`: document numbers never fall along the sequence; a document has 1 to 1024 positions.
All inputs are finite; a program needn't handle non-finite values.
Results may differ from the reference program's by a relative error of at most 0.007.
Values may be sent and summed in bfloat16 or wider, within the bound.
A program may use at most 128 MiB of HBM per device.

```python
import math
import jax
import jax.numpy as jnp
import numpy as np
from jax import lax

D = 2048
HEADS = 32
HEAD_DIM = 64
SEG = 64
LEFT = 4
REL_CLIP = 128
LAYERS = 1
TOK_DEV = 256
TOKENS = 2048
DOC_SPAN = 1024
N_SP = 8


def draw_rel_bias(key, part):
    bias_shape = (LAYERS, HEADS, 2 * REL_CLIP + 1)
    base_draw = jnp.clip(jax.random.normal(key, bias_shape, jnp.float32) * 1.5, -8.0, 8.0)
    return base_draw


def block_scale(key, dims, split, low, high):
    def one(dim, blocks):
        heights = jax.random.uniform(jax.random.fold_in(jax.random.fold_in(key, 6), dim), (blocks,), jnp.float32, low / len(split), high / len(split))
        return jnp.repeat(jnp.exp(heights), dims[dim] // blocks).reshape((-1,) + (1,) * (len(dims) - dim - 1))

    gain = one(*split[0])
    for cut in split[1:]:
        gain = gain * one(*cut)
    return gain


def profile(amount, total, bound, slope):
    portions = [(1 << 20) // math.isqrt(standing ** slope) + 1 for standing in range(2, amount + 1)]
    spare, holding = total - bound - (amount - 1), [1] * (amount - 1)
    while spare > 0:
        candidates = [i for i in range(amount - 1) if holding[i] < bound]
        mass, left = sum([portions[i] for i in candidates]), spare
        for i in candidates:
            addition = min(bound - holding[i], max(1, left * portions[i] // mass), spare)
            holding[i] = holding[i] + addition
            spare = spare - addition
    return np.array([bound] + holding)


def ragged_sizes(rng, number_of, total, limit, lean):
    if number_of == 2:
        one = jax.random.randint(rng, (), max(1, total - limit), min(limit, total - 1) + 1)
        return jnp.stack([one, total - one])
    lengths = jnp.asarray(profile(number_of, total, limit, lean), jnp.int32)
    pairs = (number_of - 1) // 2
    source_of, receiver = lengths[1:1 + 2 * pairs:2], lengths[2:2 + 2 * pairs:2]
    slack = jnp.minimum(source_of - 1, limit - receiver)
    passed = jax.random.randint(jax.random.fold_in(rng, 1), (pairs,), 0, 1 << 20) % (slack + 1)
    lengths = lengths.at[1:1 + 2 * pairs:2].set(source_of - passed).at[2:2 + 2 * pairs:2].set(receiver + passed)
    return lengths[jax.random.permutation(jax.random.fold_in(rng, 2), number_of)]


def normal_values(stream_key, extent, width, limit, shards=(), held_as=jnp.bfloat16):
    drawn = width * jax.random.normal(stream_key, extent, jnp.float32)
    if shards:
        drawn = drawn * block_scale(stream_key, extent, shards, -0.22, 0.18)
    return jnp.clip(drawn, -limit, limit).astype(held_as)


def setup_inputs(seed: int = 0) -> dict:
    keys = jax.random.split(jax.random.key(seed), 9)
    tokens = normal_values(keys[0], (TOKENS, D), 1.0, 6.0, ((0, 8),))
    documents = jnp.searchsorted(jnp.cumsum(ragged_sizes(keys[1], N_SP // 2, TOKENS, DOC_SPAN, 0)), jnp.arange(TOKENS), side="right").astype(jnp.int32)
    norm_gain = jnp.clip(1.0 + 0.18 * jax.random.normal(keys[2], (LAYERS, D), jnp.float32), 0.1, 1.9)
    w_query = normal_values(keys[3], (LAYERS, D, HEADS * HEAD_DIM), D ** -0.5, 0.125, ((1, 8), (2, 4)))
    w_key = normal_values(keys[4], (LAYERS, D, HEADS * HEAD_DIM), D ** -0.5, 0.125, ((1, 8), (2, 4)))
    w_value = normal_values(keys[5], (LAYERS, D, HEADS * HEAD_DIM), D ** -0.5, 0.125, ((1, 8), (2, 4)))
    w_out = normal_values(keys[6], (LAYERS, HEADS * HEAD_DIM, D), 0.1, 0.59765625, ((2, 8),))
    rel_bias = draw_rel_bias(jax.random.fold_in(keys[8], 71), 0)
    return dict(tokens=tokens, documents=documents, norm_gain=norm_gain, w_query=w_query, w_key=w_key, w_value=w_value, w_out=w_out, rel_bias=rel_bias)


EPS = 1e-06

def attend(queries, keys_all, values_all, query_pos, key_pos, query_doc, key_doc, bias_table):
    scores = jnp.einsum('qhe,khe->hqk', queries.astype(jnp.float32), keys_all.astype(jnp.float32)) * HEAD_DIM ** (-0.5)
    distance = jnp.clip(query_pos[:, None] - key_pos[None, :], -REL_CLIP, REL_CLIP) + REL_CLIP
    scores = scores + jnp.take(bias_table, distance, axis=1)
    query_seg = query_pos // SEG
    key_seg = key_pos // SEG
    allowed = (key_pos[None, :] >= 0) & (key_seg[None, :] <= query_seg[:, None]) & (key_seg[None, :] >= query_seg[:, None] - LEFT) & (key_doc[None, :] == query_doc[:, None])
    scores = jnp.where(allowed[None], scores, -1e+30)
    peak = lax.optimization_barrier(jnp.max(scores, axis=-1, keepdims=True))
    raised = jnp.exp(scores - peak)
    weights_bf = (raised / lax.optimization_barrier(jnp.sum(raised, axis=-1, keepdims=True))).astype(jnp.bfloat16)
    return jnp.einsum('hqk,khe->qhe', weights_bf.astype(jnp.float32), values_all.astype(jnp.float32)).astype(jnp.bfloat16)

def reference(tokens, documents, norm_gain, w_query, w_key, w_value, w_out, rel_bias):
    reach_rows = LEFT * SEG
    block_count = TOKENS // TOK_DEV
    current = tokens
    doc_pad = jnp.concatenate([jnp.zeros((reach_rows,), jnp.int32), documents.astype(jnp.int32)])
    for depth_index in range(LAYERS):
        widened = current.astype(jnp.float32)
        normed = (widened * lax.rsqrt(lax.optimization_barrier(jnp.mean(widened * widened, axis=-1, keepdims=True)) + EPS) * norm_gain[depth_index]).astype(jnp.bfloat16)
        queries = jnp.dot(normed, w_query[depth_index], preferred_element_type=jnp.float32).astype(jnp.bfloat16).reshape(TOKENS, HEADS, HEAD_DIM)
        keys_all = jnp.dot(normed, w_key[depth_index], preferred_element_type=jnp.float32).astype(jnp.bfloat16).reshape(TOKENS, HEADS, HEAD_DIM)
        values_all = jnp.dot(normed, w_value[depth_index], preferred_element_type=jnp.float32).astype(jnp.bfloat16).reshape(TOKENS, HEADS, HEAD_DIM)
        zero_rows = jnp.zeros((reach_rows, HEADS, HEAD_DIM), jnp.bfloat16)
        key_pad = jnp.concatenate([zero_rows, keys_all], axis=0)
        value_pad = jnp.concatenate([zero_rows, values_all], axis=0)
        bias_table = rel_bias[depth_index]

        def one_block(block_index):
            first_row = (block_index * TOK_DEV).astype(jnp.int32)
            query_block = lax.dynamic_slice_in_dim(queries, first_row, TOK_DEV, 0)
            key_block = lax.dynamic_slice_in_dim(key_pad, first_row, reach_rows + TOK_DEV, 0)
            value_block = lax.dynamic_slice_in_dim(value_pad, first_row, reach_rows + TOK_DEV, 0)
            query_doc = lax.dynamic_slice_in_dim(documents, first_row, TOK_DEV, 0)
            key_doc = lax.dynamic_slice_in_dim(doc_pad, first_row, reach_rows + TOK_DEV, 0)
            query_pos = first_row + jnp.arange(TOK_DEV, dtype=jnp.int32)
            key_pos = first_row - reach_rows + jnp.arange(reach_rows + TOK_DEV, dtype=jnp.int32)
            return attend(query_block, key_block, value_block, query_pos, key_pos, query_doc, key_doc, bias_table)
        attended = lax.map(one_block, jnp.arange(block_count, dtype=jnp.int32)).reshape(TOKENS, HEADS * HEAD_DIM)
        product = jnp.dot(attended, w_out[depth_index], preferred_element_type=jnp.float32)
        current = (widened + product).astype(jnp.bfloat16)
    return current
```

```python
import functools

import jax
import jax.numpy as jnp
from jax import lax
from jax.experimental import pallas as pl
from jax.experimental.pallas import tpu as pltpu
from jax.sharding import PartitionSpec as P

HEAD_DIM = 64
SEG = 64
LEFT = 4
REL_CLIP = 128


EPS = 1e-06


def passed_along(x, axis, by):
    length = lax.axis_size(axis)
    pairs = [(i, i + by) for i in range(length) if 0 <= i + by < length]
    return lax.ppermute(x, axis, pairs)


def banded_bias(bias_table, query_rows, key_rows, reach_rows):
    span_len = query_rows + key_rows - 1
    steps_back = jnp.arange(span_len, dtype=jnp.int32) - (key_rows - 1) + reach_rows
    lookup = jnp.clip(steps_back, -REL_CLIP, REL_CLIP) + REL_CLIP
    bias_line = jnp.take(bias_table, lookup, axis=1)
    reversed_line = bias_line[:, ::-1]
    repeated = jnp.tile(reversed_line, (1, query_rows))
    skewed = repeated[:, query_rows - 1 : query_rows - 1 + query_rows * (span_len - 1)]
    skewed = skewed.reshape(bias_table.shape[0], query_rows, span_len - 1)
    return skewed[:, :, :key_rows]


def attend(queries, keys_all, values_all, query_pos, key_pos, query_doc, key_doc, bias_table):
    query_rows = queries.shape[0]
    key_rows = keys_all.shape[0]
    reach_rows = key_rows - query_rows
    scores = jnp.einsum(
        "qhe,khe->hqk", queries, keys_all, preferred_element_type=jnp.float32
    ) * HEAD_DIM ** (-0.5)
    scores = scores + banded_bias(bias_table, query_rows, key_rows, reach_rows)
    query_seg = query_pos // SEG
    key_seg = key_pos // SEG
    allowed = (
        (key_pos[None, :] >= 0)
        & (key_seg[None, :] <= query_seg[:, None])
        & (key_seg[None, :] >= query_seg[:, None] - LEFT)
        & (key_doc[None, :] == query_doc[:, None])
    )
    scores = jnp.where(allowed[None], scores, -1e30)
    peak = jnp.max(scores, axis=-1, keepdims=True)
    raised = jnp.exp(scores - peak)
    weights_bf = (raised / jnp.sum(raised, axis=-1, keepdims=True)).astype(jnp.bfloat16)
    return jnp.einsum(
        "hqk,khe->qhe", weights_bf, values_all, preferred_element_type=jnp.float32
    ).astype(jnp.bfloat16)


def body(tokens, documents, norm_gain, w_query, w_key, w_value, w_out, rel_bias):
    local_rows = tokens.shape[0]
    reach_rows = LEFT * SEG
    width_local = w_query.shape[2]
    heads_local = width_local // HEAD_DIM
    offset = lax.axis_index("sp") * local_rows
    query_pos = offset + jnp.arange(local_rows, dtype=jnp.int32)
    key_pos = offset - reach_rows + jnp.arange(reach_rows + local_rows, dtype=jnp.int32)
    widened = tokens.astype(jnp.float32)
    normed = (
        widened
        * lax.rsqrt(jnp.mean(widened * widened, axis=-1, keepdims=True) + EPS)
        * norm_gain[0]
    ).astype(jnp.bfloat16)
    query_sum = jnp.dot(
        normed,
        lax.all_gather(w_query[0], "sp", axis=0, tiled=True),
        preferred_element_type=jnp.float32,
    )
    key_sum = jnp.dot(
        normed,
        lax.all_gather(w_key[0], "sp", axis=0, tiled=True),
        preferred_element_type=jnp.float32,
    )
    value_sum = jnp.dot(
        normed,
        lax.all_gather(w_value[0], "sp", axis=0, tiled=True),
        preferred_element_type=jnp.float32,
    )
    queries = query_sum.astype(jnp.bfloat16)
    keys_own = key_sum.astype(jnp.bfloat16)
    values_own = value_sum.astype(jnp.bfloat16)
    prior_keys, prior_values, prior_docs = passed_along((keys_own, values_own, documents), "sp", 1)
    keys_all = jnp.concatenate([prior_keys, keys_own], axis=0)
    values_all = jnp.concatenate([prior_values, values_own], axis=0)
    key_doc = jnp.concatenate([prior_docs, documents], axis=0)
    attended = attend(
        queries.reshape(local_rows, heads_local, HEAD_DIM),
        keys_all.reshape(reach_rows + local_rows, heads_local, HEAD_DIM),
        values_all.reshape(reach_rows + local_rows, heads_local, HEAD_DIM),
        query_pos,
        key_pos,
        documents,
        key_doc,
        rel_bias[0],
    ).reshape(local_rows, width_local)
    all_heads = lax.all_gather(attended, "tp", axis=1, tiled=True)
    return (
        widened
        + jnp.dot(
            all_heads,
            lax.all_gather(w_out[0], "sp", axis=1, tiled=True),
            preferred_element_type=jnp.float32,
        )
    ).astype(jnp.bfloat16)


MESH = pl.DeviceIdType.MESH
TOK, OUT = range(2)
UP, DOWN, ACROSS = range(3)
W0, W1, A0, A1 = range(4)
NEG = -1e30


def plane_of(t):
    c = t % 2
    return 3 * c + (t // 2) * (1 - 2 * c)


def part_for(z):
    return 2 * (((z + 1) // 2) % 2) + z // 2


def layer_kernel(
    n_sp, n_tp, doc_row, gain_ref, line_ref, x_in, wk_in, wv_in, wq_in, wo_in, out_ref,
    w_own, w_relay, w_all, wo_all, tok, resid, normed, line_all, bias, q_buf, kv_all, docs_all, mask,
    att_own, att_relay, att_all, done,
    own_sem, loc_sem, out_sem, tok_sem, res_sem, line_send, line_recv, hop_send, relay_recv, rep_send, rep_recv,
    cast_send, cast_recv, halo_send, halo_recv, tp_send, tp_recv, store_sem,
):
    rows, width = tok.shape[1:]
    depth, cols = wk_in.shape
    half_cols = cols // 2
    lanes = 2 * HEAD_DIM
    pairs = half_cols // lanes
    chunk = width // n_tp
    nz = n_sp // 2
    pieces = n_tp
    piece = rows // pieces
    s = lax.axis_index("sp")
    t = lax.axis_index("tp")
    z, x = s // 2, s % 2
    mate = s + 1 - 2 * x
    ty, tc = t // 2, t % 2
    t_core = t + 1 - 2 * tc
    t_y = (1 - ty) * 2 + tc
    t_far = (1 - ty) * 2 + 1 - tc
    home, home_y = plane_of(t), plane_of(t_y)
    first_entry, second_entry = z == home, z == home_y
    entry = first_entry | second_entry
    gap = z - home
    is_first = 1 - (gap * gap + n_sp) // (n_sp + 1)
    x_mine = x * is_first + (1 - x) * (1 - is_first)
    own_in = (wk_in, wv_in, wq_in)
    has_up, has_down = z < nz - 1, z > 0

    def at_multiple(start, size, step):
        return pl.ds(pl.multiple_of(start, step), size)

    def weight_cols(which, p):
        return at_multiple(which * half_cols + p * lanes, lanes, lanes)

    def kind_cols(kind):
        return pl.ds(kind * lanes, lanes)

    def own_copy(i, p, kind):
        which = x if i == 0 else 1 - x
        return pltpu.make_async_copy(
            own_in[kind].at[:, weight_cols(which, p)], w_own.at[i, p, :, kind_cols(kind)], own_sem.at[i, p, kind]
        )

    def local_copy(p, kind):
        return pltpu.make_async_copy(
            own_in[kind].at[:, weight_cols(x, p)],
            w_all.at[p, at_multiple(s * depth, depth, depth), kind_cols(kind)], loc_sem.at[p, kind],
        )

    def tok_copy(r):
        part = pl.ds(r * piece, piece)
        return pltpu.make_async_copy(x_in.at[part, :], tok.at[x, part, :], tok_sem.at[r])

    def out_copy(r):
        return pltpu.make_async_copy(wo_in.at[pl.ds(r * cols, cols), :], wo_all.at[2 * r + x], out_sem.at[r])

    resid_copy = pltpu.make_async_copy(x_in.at[:, at_multiple(home_y * chunk, chunk, chunk)], resid, res_sem)

    @pl.when(first_entry)
    def _():
        for r in range(pieces):
            tok_copy(r).start()

    for p in range(pairs):
        for i in (1, 0):
            for kind in range(3):
                own_copy(i, p, kind).start()

    @pl.when(first_entry)
    def _():
        for p in range(pairs):
            for kind in range(3):
                local_copy(p, kind).start()

    @pl.when(second_entry)
    def _():
        for r in range(n_tp):
            out_copy(r).start()

    resid_copy.start()

    def remote(src, dst, send, recv, **where):
        return pltpu.make_async_remote_copy(
            src_ref=src, dst_ref=dst, send_sem=send, recv_sem=recv, device_id=where, device_id_type=MESH
        )

    def slot(ch, block):
        if ch < A0:
            return w_all.at[ch - W0, at_multiple(block * depth, depth, depth), :]
        start = (block % 2) * half_cols + (ch - A0) * lanes
        return att_all.at[part_for(block // 2), :, at_multiple(start, lanes, lanes)]

    def own_ref(ch, i):
        return w_own.at[i, ch - W0] if ch < A0 else att_own.at[ch - A0, x if i == 0 else 1 - x]

    def relay_ref(ch):
        return w_relay.at[ch - W0] if ch < A0 else att_relay.at[ch - A0]

    def direct(ch):
        return remote(own_ref(ch, 0), slot(ch, s), hop_send.at[ch, 0], rep_recv.at[ch, s], sp=2 * home + x)

    def cross_in(ch):
        return remote(own_ref(ch, 1), slot(ch, s), hop_send.at[ch, 1], rep_recv.at[ch, s], sp=mate, tp=t_y)

    def cross_relay(ch):
        return remote(own_ref(ch, 1), relay_ref(ch), hop_send.at[ch, 1], relay_recv.at[ch], sp=mate, tp=t_y)

    def relay(ch):
        return remote(relay_ref(ch), slot(ch, mate), hop_send.at[ch, 2], rep_recv.at[ch, mate], sp=2 * home_y + x)

    def to_y(ch, block):
        return remote(slot(ch, block), slot(ch, block), rep_send.at[ch, 0, block], rep_recv.at[ch, block], tp=t_y)

    def to_core(ch, block):
        return remote(slot(ch, block), slot(ch, block), rep_send.at[ch, 1, block], rep_recv.at[ch, block], tp=t_core)

    def send_cross(ch):
        pl.when(first_entry)(lambda: cross_in(ch).start())
        pl.when(jnp.logical_not(first_entry))(lambda: cross_relay(ch).start())

    def send_direct(ch):
        pl.when(jnp.logical_not(first_entry))(lambda: direct(ch).start())

    def send_relay(ch):
        @pl.when(jnp.logical_not(second_entry))
        def _():
            cross_relay(ch).wait_recv()
            relay(ch).start()

    planes = [0]
    for d in range(1, nz):
        planes += [-d, d]

    def valid(off):
        return (z + off >= 0) & (z + off < nz)

    def mine(ch, off):
        @pl.when(entry & valid(off))
        def _():
            block = 2 * (z + off) + x_mine
            if off == 0:
                pl.when(jnp.logical_not(first_entry))(lambda: to_y(ch, block).wait_recv())
                if ch < A0:
                    @pl.when(first_entry)
                    def _():
                        for kind in range(3):
                            local_copy(ch - W0, kind).wait()
            else:
                to_y(ch, block).wait_recv()
            to_y(ch, block).start()
            to_core(ch, block).start()

    def theirs(ch, off):
        @pl.when(valid(off))
        def _():
            @pl.when(entry)
            def _():
                block = 2 * (z + off) + 1 - x_mine
                to_y(ch, block).wait_recv()
                to_core(ch, block).start()

            @pl.when(jnp.logical_not(entry))
            def _():
                for i in range(2):
                    to_core(ch, 2 * (z + off) + i).wait_recv()

    def spread(ch, first, last):
        for i in range(first, last + 1):
            if i < len(planes):
                mine(ch, planes[i])
            if i > 0:
                theirs(ch, planes[i - 1])

    def drain(ch):
        pl.when(jnp.logical_not(first_entry))(lambda: direct(ch).wait_send())
        cross_relay(ch).wait_send()
        pl.when(jnp.logical_not(second_entry))(lambda: relay(ch).wait_send())

        @pl.when(entry)
        def _():
            for zz in range(nz):
                to_y(ch, 2 * zz + x_mine).wait_send()
                for i in range(2):
                    to_core(ch, 2 * zz + i).wait_send()

    def cast_ref(kind, which, r):
        if kind == OUT:
            return wo_all.at[2 * r + which]
        if r == pieces:
            return docs_all.at[:, at_multiple((1 + which) * rows, rows, rows)]
        return tok.at[which, pl.ds(r * piece, piece), :]

    def move(kind, way, r, src=None):
        ref = cast_ref(kind, x, r)
        return remote(
            ref if src is None else src, ref, cast_send.at[kind, way, r], cast_recv.at[kind, x, r],
            sp=(s + 2, s - 2, mate)[way],
        )

    def across_in(kind, r):
        ref = cast_ref(kind, 1 - x, r)
        return remote(ref, ref, cast_send.at[kind, ACROSS, r], cast_recv.at[kind, 1 - x, r], sp=mate)

    centers = (home, home_y)

    def cast_send_on(kind, r, src=None):
        pl.when((z >= centers[kind]) & has_up)(lambda: move(kind, UP, r, src).start())
        pl.when((z <= centers[kind]) & has_down)(lambda: move(kind, DOWN, r, src).start())
        move(kind, ACROSS, r, src).start()

    def cast_source(kind, r):
        if r == pieces and kind == TOK:
            docs_all[:, at_multiple((1 + x) * rows, rows, rows)] = doc_row[...]
            cast_send_on(kind, r, doc_row)
            return
        (tok_copy, out_copy)[kind](r).wait()
        cast_send_on(kind, r)

    def cast_forward(kind, r):
        @pl.when(z != centers[kind])
        def _():
            move(kind, UP, r).wait_recv()
            cast_send_on(kind, r)

    def cast_drain(kind, count):
        for r in range(count):
            pl.when((z >= centers[kind]) & has_up)(lambda: move(kind, UP, r).wait_send())
            pl.when((z <= centers[kind]) & has_down)(lambda: move(kind, DOWN, r).wait_send())
            move(kind, ACROSS, r).wait_send()

    line_targets = (t_core, t_y, t_far)

    def line_copy(i):
        return remote(line_ref, line_all, line_send.at[i], line_recv, tp=line_targets[i])

    has_next, has_prev = home < nz - 1, home > 0

    def halo(i):
        if i == pairs:
            src, dst = docs_all.at[:, pl.ds(2 * rows, rows)], docs_all.at[:, pl.ds(0, rows)]
        else:
            src, dst = kv_all.at[i, pl.ds(2 * rows, rows), :], kv_all.at[i, pl.ds(0, rows), :]
        return remote(src, dst, halo_send.at[i], halo_recv.at[i], tp=part_for((home + 1) % nz))

    barrier = pltpu.get_barrier_semaphore()
    for d in range(1, nz):
        pl.semaphore_signal(
            barrier, inc=1, device_id={"sp": lax.rem(s + 2 * d, n_sp)}, device_id_type=MESH
        )
    for peer in (t_core, t_y, t_far):
        pl.semaphore_signal(barrier, inc=1, device_id={"tp": peer}, device_id_type=MESH)
    for peer in (t, t_y):
        pl.semaphore_signal(barrier, inc=1, device_id={"sp": mate, "tp": peer}, device_id_type=MESH)
    pl.semaphore_wait(barrier, nz + 4)

    @pl.when(first_entry)
    def _():
        cast_source(TOK, pieces)
        cast_source(TOK, 0)

    for p in range(pairs):
        for i in (1, 0):
            for kind in range(3):
                own_copy(i, p, kind).wait()
            (send_direct, send_cross)[i](W0 + p)

    @pl.when(first_entry)
    def _():
        for r in range(1, pieces):
            cast_source(TOK, r)
        for i in range(3):
            line_copy(i).start()

    @pl.when(has_prev == False)
    def _():
        docs_all[:, pl.ds(0, rows)] = jnp.full((8, rows), -1, jnp.int32)
        for p in range(pairs):
            kv_all[p, pl.ds(0, rows), :] = jnp.zeros((rows, 2 * lanes), jnp.bfloat16)

    send_relay(W0)
    cast_forward(TOK, pieces)
    cast_forward(TOK, 0)
    send_relay(W1)
    spread(W0, 0, 0)
    cast_forward(TOK, 1)
    spread(W0, 1, 2)
    cast_forward(TOK, 2)
    spread(W0, 3, 4)
    cast_forward(TOK, 3)
    spread(W0, 5, 7)

    def normalize(which):
        wide = tok[which].astype(jnp.float32)
        normed[at_multiple(which * rows, rows, rows), :] = (
            wide * lax.rsqrt(jnp.mean(wide * wide, axis=-1, keepdims=True) + EPS) * gain_ref[...]
        ).astype(jnp.bfloat16)

    normalize(x)
    spread(W1, 0, 2)

    q_rows, span = 2 * SEG, (LEFT + 2) * SEG
    heads = half_cols // HEAD_DIM
    blocks = 2 * rows // q_rows

    pl.when(first_entry)(lambda: line_all.__setitem__(Ellipsis, line_ref[...]))
    pl.when(jnp.logical_not(first_entry))(lambda: line_copy(0).wait_recv())
    q_seg = lax.broadcasted_iota(jnp.int32, (q_rows, span), 0) // SEG
    k_seg = lax.broadcasted_iota(jnp.int32, (q_rows, span), 1) // SEG
    near = (k_seg >= q_seg) & (k_seg <= q_seg + LEFT)
    for h in range(heads):
        line = jnp.broadcast_to(line_all[pl.ds(x * heads + h, 1), :], (q_rows, line_ref.shape[1]))
        skew = pltpu.roll(line, 0, 1, stride=1, stride_axis=0)
        bias[h] = jnp.where(near, skew[:, :span], NEG)

    for r in range(pieces + 1):
        across_in(TOK, r).wait_recv()
    normalize(1 - x)
    pl.when(has_next)(lambda: halo(pairs).start())
    spread(W1, 3, 5)

    @pl.when(second_entry)
    def _():
        for r in range(n_tp):
            cast_source(OUT, r)

    def project(p):
        made = jnp.dot(normed[...], w_all[p], preferred_element_type=jnp.float32).astype(jnp.bfloat16)
        kv_all[p, pl.ds(rows, 2 * rows), :] = made[:, : 2 * lanes]
        q_buf[p] = (made[:, 2 * lanes :].astype(jnp.float32) * HEAD_DIM ** (-0.5)).astype(jnp.bfloat16)
        pl.when(has_next)(lambda: halo(p).start())

    project(0)
    spread(W1, 6, 7)
    project(1)

    low = lax.broadcasted_iota(jnp.int32, (q_rows, lanes), 1) < HEAD_DIM
    eye = lax.broadcasted_iota(jnp.int32, (q_rows, q_rows), 0) == lax.broadcasted_iota(jnp.int32, (q_rows, q_rows), 1)

    def make_mask(j):
        q_docs = docs_all[pl.ds(0, 1), pl.ds(rows + j * q_rows, q_rows)].astype(jnp.float32)
        k_docs = docs_all[pl.ds(0, 1), pl.ds(j * q_rows, span)].astype(jnp.float32)
        column = jnp.sum(jnp.where(eye, jnp.broadcast_to(q_docs, (q_rows, q_rows)), 0.0), axis=1, keepdims=True)
        mask[j] = jnp.where(column == k_docs, 0.0, NEG)

    def attend_rows(p, j):
        keys = pl.ds(j * q_rows, span)
        q_pair = q_buf[p, pl.ds(j * q_rows, q_rows), :]
        k_pair = kv_all[p, keys, pl.ds(0, lanes)]
        v_pair = kv_all[p, keys, pl.ds(lanes, lanes)]
        both = []
        for half in range(2):
            on = low if half == 0 else jnp.logical_not(low)
            q_one = jnp.where(on, q_pair, jnp.zeros_like(q_pair))
            score = lax.dot_general(q_one, k_pair, (((1,), (1,)), ((), ())), preferred_element_type=jnp.float32)
            score = score + bias[2 * p + half] + mask[j]
            raised = jnp.exp(score - jnp.max(score, axis=-1, keepdims=True))
            total = jnp.sum(raised, axis=-1, keepdims=True)
            both.append(jnp.dot(raised.astype(jnp.bfloat16), v_pair, preferred_element_type=jnp.float32) / total)
        return jnp.where(low, both[0], both[1]).astype(jnp.bfloat16)

    per = blocks // 2

    def attend_half(p, which):
        for j in range(per):
            found = attend_rows(p, which * per + j)
            part = pl.ds(j * q_rows, q_rows)
            att_own[p, which, part, :] = found

            @pl.when(first_entry & (x == which))
            def _():
                att_all[t, part, at_multiple(x * half_cols + p * lanes, lanes, lanes)] = found

        pl.when(x == which)(lambda: send_direct(A0 + p))
        pl.when(x != which)(lambda: send_cross(A0 + p))

    for j in range(per, blocks):
        make_mask(j)
    attend_half(0, 1)

    @pl.when(has_prev)
    def _():
        for i in (pairs, 0):
            halo(i).wait_recv()

    for j in range(per):
        make_mask(j)
    cast_forward(OUT, 0)
    attend_half(0, 0)
    cast_forward(OUT, 1)
    send_relay(A0)
    attend_half(1, 1)
    cast_forward(OUT, 2)
    pl.when(has_prev)(lambda: halo(1).wait_recv())
    attend_half(1, 0)
    cast_forward(OUT, 3)
    send_relay(A1)
    spread(A0, 0, 7)
    spread(A1, 0, 7)
    for r in range(n_tp):
        across_in(OUT, r).wait_recv()
    resid_copy.wait()
    half_chunk = chunk // 2
    for i in range(2):
        made = jnp.zeros((rows, half_chunk), jnp.float32)
        for r in range(n_tp):
            made = made + jnp.dot(att_all[r], wo_all[2 * r + i], preferred_element_type=jnp.float32)
        part = pl.ds(i * half_chunk, half_chunk)
        done[home_y, :, part] = (resid[:, part].astype(jnp.float32) + made).astype(jnp.bfloat16)

    def store(which):
        return pltpu.make_async_copy(
            done.at[which], out_ref.at[:, at_multiple(which * chunk, chunk, chunk)], store_sem.at[which]
        )

    def tp_move(i, which, target):
        return remote(done.at[which], done.at[which], tp_send.at[i], tp_recv.at[i], tp=target)

    out_to_y, out_to_core, pass_on = tp_move(0, home_y, t_y), tp_move(1, home_y, t_core), tp_move(2, home, t_core)
    out_to_y.start()
    out_to_core.start()
    store(home_y).start()
    out_to_y.wait_recv()
    pass_on.start()
    store(home).start()
    out_to_core.wait_recv()
    store(plane_of(t_far)).start()
    pass_on.wait_recv()
    store(plane_of(t_core)).start()
    for which in range(n_tp):
        store(which).wait()

    for ch in range(4):
        drain(ch)
    cast_drain(TOK, pieces + 1)
    cast_drain(OUT, n_tp)

    @pl.when(first_entry)
    def _():
        for i in range(3):
            line_copy(i).wait_send()

    @pl.when(has_next)
    def _():
        for i in range(pairs + 1):
            halo(i).wait_send()
    for one in (out_to_y, out_to_core, pass_on):
        one.wait_send()


def body_one(n_sp, n_tp, tokens, documents, norm_gain, w_query, w_key, w_value, w_out, rel_bias):
    rows, width = tokens.shape
    depth, cols = w_query.shape[1:]
    heads = cols // HEAD_DIM
    out_cols = w_out.shape[2]
    chunk = width // n_tp
    lanes = 2 * HEAD_DIM
    pairs = cols // 2 // lanes
    reach = LEFT * SEG
    table = rel_bias[0]
    furthest = table[:, 2 * REL_CLIP:]
    ahead, behind = reach - REL_CLIP, reach - REL_CLIP - 1
    line = jnp.concatenate(
        [
            jnp.broadcast_to(furthest, (heads, ahead)),
            table[:, ::-1],
            jnp.broadcast_to(furthest, (heads, behind)),
        ],
        axis=1,
    )
    doc_row = jnp.broadcast_to(documents[None, :], (8, rows))
    bf, f32 = jnp.bfloat16, jnp.float32
    vmem = pl.BlockSpec(memory_space=pltpu.VMEM)
    hbm = pl.BlockSpec(memory_space=pl.ANY)
    dma = pltpu.SemaphoreType.DMA
    q_rows, span = 2 * SEG, (LEFT + 2) * SEG
    return pl.pallas_call(
        functools.partial(layer_kernel, n_sp, n_tp),
        out_shape=jax.ShapeDtypeStruct((rows, width), bf),
        in_specs=[vmem] * 3 + [hbm] * 5,
        out_specs=hbm,
        scratch_shapes=[
            pltpu.VMEM((2, pairs, depth, 3 * lanes), bf),
            pltpu.VMEM((pairs, depth, 3 * lanes), bf),
            pltpu.VMEM((pairs, n_sp * depth, 3 * lanes), bf),
            pltpu.VMEM((n_sp, cols, out_cols), bf),
            pltpu.VMEM((2, rows, width), bf),
            pltpu.VMEM((rows, chunk), bf),
            pltpu.VMEM((2 * rows, width), bf),
            pltpu.VMEM(line.shape, f32),
            pltpu.VMEM((heads // 2, q_rows, span), f32),
            pltpu.VMEM((pairs, 2 * rows, lanes), bf),
            pltpu.VMEM((pairs, 3 * rows, 2 * lanes), bf),
            pltpu.VMEM((8, 3 * rows), jnp.int32),
            pltpu.VMEM((2 * rows // q_rows, q_rows, span), f32),
            pltpu.VMEM((pairs, 2, rows, lanes), bf),
            pltpu.VMEM((pairs, rows, lanes), bf),
            pltpu.VMEM((n_tp, rows, cols), bf),
            pltpu.VMEM((n_tp, rows, chunk), bf),
            dma((2, pairs, 3)),
            dma((pairs, 3)),
            dma((n_tp,)),
            dma((n_tp,)),
            dma(()),
            dma((3,)),
            dma(()),
            dma((4, 3)),
            dma((4,)),
            dma((4, 2, n_sp)),
            dma((4, n_sp)),
            dma((2, 3, n_tp + 1)),
            dma((2, 2, n_tp + 1)),
            dma((pairs + 1,)),
            dma((pairs + 1,)),
            dma((3,)),
            dma((3,)),
            dma((n_tp,)),
        ],
        compiler_params=pltpu.CompilerParams(
            collective_id=0, has_side_effects=True, vmem_limit_bytes=60 * 1024 * 1024
        ),
    )(doc_row, norm_gain, line, tokens, w_key[0], w_value[0], w_query[0], w_out[0])


def fits_one(mesh):
    return mesh.shape["tp"] == 4 and mesh.shape["sp"] == 2 * mesh.shape["tp"]


def solution(mesh):
    n_sp, n_tp = mesh.shape["sp"], mesh.shape["tp"]
    run = functools.partial(body_one, n_sp, n_tp) if fits_one(mesh) else body
    in_specs = (
        P("sp", None),
        P("sp"),
        P(),
        P(None, "sp", "tp"),
        P(None, "sp", "tp"),
        P(None, "sp", "tp"),
        P(None, None, "sp"),
        P(None, "tp", None),
    )
    out_specs = P("sp", None)
    return jax.shard_map(run, mesh=mesh, in_specs=in_specs, out_specs=out_specs, check_vma=False)
```

```python
import functools

import jax
import jax.numpy as jnp
from jax import lax
from jax.experimental import pallas as pl
from jax.experimental.pallas import tpu as pltpu
from jax.sharding import PartitionSpec as P

HEAD_DIM = 64
SEG = 64
LEFT = 4
REL_CLIP = 128


EPS = 1e-06


def passed_along(x, axis, by):
    length = lax.axis_size(axis)
    pairs = [(i, i + by) for i in range(length) if 0 <= i + by < length]
    return lax.ppermute(x, axis, pairs)


def banded_bias(bias_table, query_rows, key_rows, reach_rows):
    span_len = query_rows + key_rows - 1
    steps_back = jnp.arange(span_len, dtype=jnp.int32) - (key_rows - 1) + reach_rows
    lookup = jnp.clip(steps_back, -REL_CLIP, REL_CLIP) + REL_CLIP
    bias_line = jnp.take(bias_table, lookup, axis=1)
    reversed_line = bias_line[:, ::-1]
    repeated = jnp.tile(reversed_line, (1, query_rows))
    skewed = repeated[:, query_rows - 1 : query_rows - 1 + query_rows * (span_len - 1)]
    skewed = skewed.reshape(bias_table.shape[0], query_rows, span_len - 1)
    return skewed[:, :, :key_rows]


def attend(queries, keys_all, values_all, query_pos, key_pos, query_doc, key_doc, bias_table):
    query_rows = queries.shape[0]
    key_rows = keys_all.shape[0]
    reach_rows = key_rows - query_rows
    scores = jnp.einsum(
        "qhe,khe->hqk", queries, keys_all, preferred_element_type=jnp.float32
    ) * HEAD_DIM ** (-0.5)
    scores = scores + banded_bias(bias_table, query_rows, key_rows, reach_rows)
    query_seg = query_pos // SEG
    key_seg = key_pos // SEG
    allowed = (
        (key_pos[None, :] >= 0)
        & (key_seg[None, :] <= query_seg[:, None])
        & (key_seg[None, :] >= query_seg[:, None] - LEFT)
        & (key_doc[None, :] == query_doc[:, None])
    )
    scores = jnp.where(allowed[None], scores, -1e30)
    peak = jnp.max(scores, axis=-1, keepdims=True)
    raised = jnp.exp(scores - peak)
    weights_bf = (raised / jnp.sum(raised, axis=-1, keepdims=True)).astype(jnp.bfloat16)
    return jnp.einsum(
        "hqk,khe->qhe", weights_bf, values_all, preferred_element_type=jnp.float32
    ).astype(jnp.bfloat16)


def body(tokens, documents, norm_gain, w_query, w_key, w_value, w_out, rel_bias):
    local_rows = tokens.shape[0]
    reach_rows = LEFT * SEG
    width_local = w_query.shape[2]
    heads_local = width_local // HEAD_DIM
    offset = lax.axis_index("sp") * local_rows
    query_pos = offset + jnp.arange(local_rows, dtype=jnp.int32)
    key_pos = offset - reach_rows + jnp.arange(reach_rows + local_rows, dtype=jnp.int32)
    widened = tokens.astype(jnp.float32)
    normed = (
        widened
        * lax.rsqrt(jnp.mean(widened * widened, axis=-1, keepdims=True) + EPS)
        * norm_gain[0]
    ).astype(jnp.bfloat16)
    query_sum = jnp.dot(
        normed,
        lax.all_gather(w_query[0], "sp", axis=0, tiled=True),
        preferred_element_type=jnp.float32,
    )
    key_sum = jnp.dot(
        normed,
        lax.all_gather(w_key[0], "sp", axis=0, tiled=True),
        preferred_element_type=jnp.float32,
    )
    value_sum = jnp.dot(
        normed,
        lax.all_gather(w_value[0], "sp", axis=0, tiled=True),
        preferred_element_type=jnp.float32,
    )
    queries = query_sum.astype(jnp.bfloat16)
    keys_own = key_sum.astype(jnp.bfloat16)
    values_own = value_sum.astype(jnp.bfloat16)
    prior_keys, prior_values, prior_docs = passed_along((keys_own, values_own, documents), "sp", 1)
    keys_all = jnp.concatenate([prior_keys, keys_own], axis=0)
    values_all = jnp.concatenate([prior_values, values_own], axis=0)
    key_doc = jnp.concatenate([prior_docs, documents], axis=0)
    attended = attend(
        queries.reshape(local_rows, heads_local, HEAD_DIM),
        keys_all.reshape(reach_rows + local_rows, heads_local, HEAD_DIM),
        values_all.reshape(reach_rows + local_rows, heads_local, HEAD_DIM),
        query_pos,
        key_pos,
        documents,
        key_doc,
        rel_bias[0],
    ).reshape(local_rows, width_local)
    all_heads = lax.all_gather(attended, "tp", axis=1, tiled=True)
    return (
        widened
        + jnp.dot(
            all_heads,
            lax.all_gather(w_out[0], "sp", axis=1, tiled=True),
            preferred_element_type=jnp.float32,
        )
    ).astype(jnp.bfloat16)


MESH = pl.DeviceIdType.MESH
TOK, OUT = range(2)
UP, DOWN, ACROSS = range(3)
W0, W1, A0, A1 = range(4)
NEG = -1e30


def plane_of(t):
    c = t % 2
    return 3 * c + (t // 2) * (1 - 2 * c)


def part_for(z):
    return 2 * (((z + 1) // 2) % 2) + z // 2


def layer_kernel(
    n_sp, n_tp, doc_in, gain_in, table_in, x_in, wk_in, wv_in, wq_in, wo_in, out_ref,
    w_own, w_relay, w_all, wo_all, tok, aid, wo_aid, resid, normed, gain, table, bias, q_buf, kv_all, docs_all, mask,
    att_own, att_relay, att_all, done,
    own_sem, loc_sem, out_sem, tok_sem, aid_sem, aid_send, wo_aid_sem, wo_aid_send, res_sem, small_sem, line_send, line_recv, hop_send, relay_recv, rep_send, rep_recv,
    cast_send, cast_recv, halo_send, halo_recv, tp_send, tp_recv, store_sem,
):
    rows, width = tok.shape[1:]
    depth, cols = wk_in.shape
    half_cols = cols // 2
    lanes = 2 * HEAD_DIM
    pairs = half_cols // lanes
    chunk = width // n_tp
    nz = n_sp // 2
    pieces = n_tp
    piece = rows // pieces
    s = lax.axis_index("sp")
    t = lax.axis_index("tp")
    z, x = s // 2, s % 2
    mate = s + 1 - 2 * x
    ty, tc = t // 2, t % 2
    t_core = t + 1 - 2 * tc
    t_y = (1 - ty) * 2 + tc
    t_far = (1 - ty) * 2 + 1 - tc
    home, home_y = plane_of(t), plane_of(t_y)
    first_entry, second_entry = z == home, z == home_y
    entry = first_entry | second_entry
    gap = z - home
    is_first = 1 - (gap * gap + n_sp) // (n_sp + 1)
    x_mine = x * is_first + (1 - x) * (1 - is_first)
    own_in = (wk_in, wv_in, wq_in)
    has_up, has_down = z < nz - 1, z > 0

    def at_multiple(start, size, step):
        return pl.ds(pl.multiple_of(start, step), size)

    def weight_cols(which, p):
        return at_multiple(which * half_cols + p * lanes, lanes, lanes)

    def kind_cols(kind):
        return pl.ds(kind * lanes, lanes)

    def own_copy(i, p, kind):
        which = x if i == 0 else 1 - x
        return pltpu.make_async_copy(
            own_in[kind].at[:, weight_cols(which, p)], w_own.at[i, p, :, kind_cols(kind)], own_sem.at[i, p, kind]
        )

    def local_copy(p, kind):
        return pltpu.make_async_copy(
            own_in[kind].at[:, weight_cols(x, p)],
            w_all.at[p, at_multiple(s * depth, depth, depth), kind_cols(kind)], loc_sem.at[p, kind],
        )

    def tok_copy(r):
        part = pl.ds(r * piece, piece)
        return pltpu.make_async_copy(x_in.at[part, :], tok.at[x, part, :], tok_sem.at[r])

    def out_copy(r):
        return pltpu.make_async_copy(wo_in.at[pl.ds(r * cols, cols), :], wo_all.at[2 * r + x], out_sem.at[r])

    doc_copy = pltpu.make_async_copy(doc_in, docs_all.at[:, at_multiple((1 + x) * rows, rows, rows)], small_sem.at[0])
    gain_copy = pltpu.make_async_copy(gain_in, gain, small_sem.at[1])
    table_copy = pltpu.make_async_copy(table_in, table, small_sem.at[2])
    resid_copy = pltpu.make_async_copy(x_in.at[:, at_multiple(home_y * chunk, chunk, chunk)], resid, res_sem)

    gain_copy.start()

    @pl.when(first_entry)
    def _():
        doc_copy.start()
        for r in range(pieces):
            tok_copy(r).start()
        table_copy.start()

    for p in range(pairs):
        for i in (1, 0):
            for kind in range(3):
                own_copy(i, p, kind).start()

    @pl.when(first_entry)
    def _():
        for p in range(pairs):
            for kind in range(3):
                local_copy(p, kind).start()

    outer = (z == 0) | (z == nz - 1)
    inner = jnp.logical_not(outer)
    lower = z < nz // 2
    aid_copy = pltpu.make_async_copy(x_in.at[pl.ds(rows // 2, rows // 2), :], aid, aid_sem)

    def wo_aid_copy(r):
        i = r - n_tp // 2
        return pltpu.make_async_copy(wo_in.at[pl.ds(r * cols, cols), :], wo_aid.at[i], wo_aid_sem.at[i])

    @pl.when(first_entry & inner)
    def _():
        for r in range(n_tp // 2, n_tp):
            wo_aid_copy(r).start()

    @pl.when(second_entry)
    def _():
        pl.when(inner)(lambda: aid_copy.start())

        for r in range(n_tp):
            out_copy(r).start()

    resid_copy.start()

    def remote(src, dst, send, recv, **where):
        return pltpu.make_async_remote_copy(
            src_ref=src, dst_ref=dst, send_sem=send, recv_sem=recv, device_id=where, device_id_type=MESH
        )

    def slot(ch, block):
        if ch < A0:
            return w_all.at[ch - W0, at_multiple(block * depth, depth, depth), :]
        start = (block % 2) * half_cols + (ch - A0) * lanes
        return att_all.at[part_for(block // 2), :, at_multiple(start, lanes, lanes)]

    def own_ref(ch, i):
        return w_own.at[i, ch - W0] if ch < A0 else att_own.at[ch - A0, x if i == 0 else 1 - x]

    def relay_ref(ch):
        return w_relay.at[ch - W0] if ch < A0 else att_relay.at[ch - A0]

    def direct(ch):
        return remote(own_ref(ch, 0), slot(ch, s), hop_send.at[ch, 0], rep_recv.at[ch, s], sp=2 * home + x)

    def cross_in(ch):
        return remote(own_ref(ch, 1), slot(ch, s), hop_send.at[ch, 1], rep_recv.at[ch, s], sp=mate, tp=t_y)

    def cross_relay(ch):
        return remote(own_ref(ch, 1), relay_ref(ch), hop_send.at[ch, 1], relay_recv.at[ch], sp=mate, tp=t_y)

    def relay(ch):
        return remote(relay_ref(ch), slot(ch, mate), hop_send.at[ch, 2], rep_recv.at[ch, mate], sp=2 * home_y + x)

    def to_y(ch, block):
        return remote(slot(ch, block), slot(ch, block), rep_send.at[ch, 0, block], rep_recv.at[ch, block], tp=t_y)

    def to_core(ch, block):
        return remote(slot(ch, block), slot(ch, block), rep_send.at[ch, 1, block], rep_recv.at[ch, block], tp=t_core)

    def send_cross(ch):
        pl.when(first_entry)(lambda: cross_in(ch).start())
        pl.when(jnp.logical_not(first_entry))(lambda: cross_relay(ch).start())

    def send_direct(ch):
        pl.when(jnp.logical_not(first_entry))(lambda: direct(ch).start())

    def send_relay(ch):
        @pl.when(jnp.logical_not(second_entry))
        def _():
            cross_relay(ch).wait_recv()
            relay(ch).start()

    planes = [0]
    for d in range(1, nz):
        planes += [-d, d]

    def valid(off):
        return (z + off >= 0) & (z + off < nz)

    def mine(ch, off):
        @pl.when(entry & valid(off))
        def _():
            block = 2 * (z + off) + x_mine
            if off == 0:
                pl.when(jnp.logical_not(first_entry))(lambda: to_y(ch, block).wait_recv())
                if ch < A0:
                    @pl.when(first_entry)
                    def _():
                        for kind in range(3):
                            local_copy(ch - W0, kind).wait()
            else:
                to_y(ch, block).wait_recv()
            to_y(ch, block).start()
            to_core(ch, block).start()

    def theirs(ch, off):
        @pl.when(valid(off))
        def _():
            @pl.when(entry)
            def _():
                block = 2 * (z + off) + 1 - x_mine
                to_y(ch, block).wait_recv()
                to_core(ch, block).start()

            @pl.when(jnp.logical_not(entry))
            def _():
                for i in range(2):
                    to_core(ch, 2 * (z + off) + i).wait_recv()

    def spread(ch, first, last):
        for i in range(first, last + 1):
            if i < len(planes):
                mine(ch, planes[i])
            if i > 0:
                theirs(ch, planes[i - 1])

    def drain(ch):
        pl.when(jnp.logical_not(first_entry))(lambda: direct(ch).wait_send())
        cross_relay(ch).wait_send()
        pl.when(jnp.logical_not(second_entry))(lambda: relay(ch).wait_send())

        @pl.when(entry)
        def _():
            for zz in range(nz):
                to_y(ch, 2 * zz + x_mine).wait_send()
                for i in range(2):
                    to_core(ch, 2 * zz + i).wait_send()

    def cast_ref(kind, which, r):
        if kind == OUT:
            return wo_all.at[2 * r + which]
        if r == pieces:
            return docs_all.at[:, at_multiple((1 + which) * rows, rows, rows)]
        return tok.at[which, pl.ds(r * piece, piece), :]

    def move(kind, way, r, src=None):
        ref = cast_ref(kind, x, r)
        return remote(
            ref if src is None else src, ref, cast_send.at[kind, way, r], cast_recv.at[kind, x, r],
            sp=(s + 2, s - 2, mate)[way],
        )

    def across_in(kind, r):
        ref = cast_ref(kind, 1 - x, r)
        return remote(ref, ref, cast_send.at[kind, ACROSS, r], cast_recv.at[kind, 1 - x, r], sp=mate)

    centers = (home, home_y)

    def aided(kind, r):
        return pieces // 2 <= r < pieces

    def goes(kind, way, r):
        ok = (z >= centers[kind]) & has_up if way == UP else (z <= centers[kind]) & has_down
        if aided(kind, r):
            near = jnp.logical_not(lower) if way == UP else lower
            ok = ok & jnp.logical_not((z == centers[kind]) & inner & near)
        return ok

    def aid_send_on(r):
        part = pl.ds((r - pieces // 2) * piece, piece)
        return remote(
            aid.at[part, :], cast_ref(TOK, x, r), aid_send.at[r - pieces // 2], cast_recv.at[TOK, x, r],
            sp=s + 2 - 4 * (1 - z // (nz // 2)), tp=t_y,
        )

    def wo_aid_send_on(r):
        i = r - n_tp // 2
        return remote(
            wo_aid.at[i], cast_ref(OUT, x, r), wo_aid_send.at[i], cast_recv.at[OUT, x, r],
            sp=s + 2 - 4 * (1 - z // (nz // 2)), tp=t_y,
        )

    def cast_along(kind, r, src=None):
        for way in (UP, DOWN):
            pl.when(goes(kind, way, r))(lambda: move(kind, way, r, src).start())

    def cast_send_on(kind, r, src=None):
        cast_along(kind, r, src)
        move(kind, ACROSS, r, src).start()

    def cast_source(kind, r):
        if r == pieces and kind == TOK:
            doc_copy.wait()
            cast_send_on(kind, r)
            return
        (tok_copy, out_copy)[kind](r).wait()
        cast_send_on(kind, r)

    def cast_forward(kind, r):
        @pl.when(z != centers[kind])
        def _():
            move(kind, UP, r).wait_recv()
            cast_send_on(kind, r)

    def cast_drain(kind, count):
        for r in range(count):
            for way in (UP, DOWN):
                pl.when(goes(kind, way, r))(lambda: move(kind, way, r).wait_send())
            move(kind, ACROSS, r).wait_send()

    line_targets = (t_core, t_y, t_far)

    def line_copy(i):
        return remote(table, table, line_send.at[i], line_recv, tp=line_targets[i])

    has_next, has_prev = home < nz - 1, home > 0

    def halo(i):
        if i == pairs:
            src, dst = docs_all.at[:, pl.ds(2 * rows, rows)], docs_all.at[:, pl.ds(0, rows)]
        else:
            src, dst = kv_all.at[i, pl.ds(2 * rows, rows), :], kv_all.at[i, pl.ds(0, rows), :]
        return remote(src, dst, halo_send.at[i], halo_recv.at[i], tp=part_for((home + 1) % nz))

    barrier = pltpu.get_barrier_semaphore()
    for d in range(1, nz):
        pl.semaphore_signal(
            barrier, inc=1, device_id={"sp": lax.rem(s + 2 * d, n_sp)}, device_id_type=MESH
        )
    for peer in (t_core, t_y, t_far):
        pl.semaphore_signal(barrier, inc=1, device_id={"tp": peer}, device_id_type=MESH)
    for peer in (t, t_y):
        pl.semaphore_signal(barrier, inc=1, device_id={"sp": mate, "tp": peer}, device_id_type=MESH)
    pl.semaphore_signal(
        barrier, inc=1, device_id={"sp": s + 2 - 4 * (z % 2), "tp": t_y}, device_id_type=MESH
    )
    pl.semaphore_wait(barrier, nz + 5)

    for p in range(pairs):
        for i in (1, 0):
            for kind in range(3):
                own_copy(i, p, kind).wait()
            (send_direct, send_cross)[i](W0 + p)

    @pl.when(first_entry)
    def _():
        for r in (pieces,) + tuple(range(pieces // 2)):
            cast_source(TOK, r)
        table_copy.wait()
        for i in range(3):
            line_copy(i).start()

    def out_along(r):
        out_copy(r).wait()
        cast_along(OUT, r)

    def out_near(r):
        pl.when(goes(OUT, UP, r) & jnp.logical_not(lower))(lambda: move(OUT, UP, r).start())
        pl.when(goes(OUT, DOWN, r) & lower)(lambda: move(OUT, DOWN, r).start())

    def out_far(r):
        pl.when(goes(OUT, UP, r) & lower)(lambda: move(OUT, UP, r).start())
        pl.when(goes(OUT, DOWN, r) & jnp.logical_not(lower))(lambda: move(OUT, DOWN, r).start())

    def out_across(r):
        move(OUT, ACROSS, r).start()

    def out_pass(r):
        @pl.when(z != home_y)
        def _():
            move(OUT, UP, r).wait_recv()
            cast_along(OUT, r)

    @pl.when(second_entry)
    def _():
        @pl.when(inner)
        def _():
            aid_copy.wait()
            for r in range(pieces // 2, pieces):
                aid_send_on(r).start()

        @pl.when(outer)
        def _():
            for r in range(n_tp):
                out_along(r)
            out_across(0)

    @pl.when(has_prev == False)
    def _():
        docs_all[:, pl.ds(0, rows)] = jnp.full((1, rows), -1, jnp.int32)
        for p in range(pairs):
            kv_all[p, pl.ds(0, rows), :] = jnp.zeros((rows, 2 * lanes), jnp.bfloat16)

    def around(d):
        return (0,) if d == 0 else (-d, d)

    def pass_mine(ch, d):
        for off in around(d):
            mine(ch, off)

    def pass_theirs(ch, d):
        for off in around(d):
            theirs(ch, off)

    @pl.when(first_entry)
    def _():
        pass_mine(W0, 0)
        pass_mine(W1, 0)
        send_relay(W0)
        send_relay(W1)
        for r in range(pieces // 2, pieces):
            cast_source(TOK, r)
        for ch in (W0, W1):
            for d in range(1, nz):
                pass_mine(ch, d)

        @pl.when(inner)
        def _():
            for r in range(n_tp):
                out_pass(r)

        for ch in (W0, W1):
            for d in range(nz):
                pass_theirs(ch, d)

    @pl.when(second_entry)
    def _():
        pass_mine(W0, 0)
        cast_forward(TOK, pieces)
        cast_forward(TOK, 0)
        pass_mine(W1, 0)
        cast_forward(TOK, 1)
        pass_mine(W0, 1)
        pass_mine(W1, 1)
        cast_forward(TOK, 2)
        pass_mine(W0, 2)
        pass_mine(W1, 2)
        cast_forward(TOK, 3)
        pass_mine(W0, 3)
        pass_mine(W1, 3)

        @pl.when(inner)
        def _():
            for r in range(n_tp):
                out_copy(r).wait()
                out_far(r)
            out_across(0)

        for ch in (W0, W1):
            for d in range(nz):
                pass_theirs(ch, d)

    @pl.when(jnp.logical_not(entry))
    def _():
        send_relay(W0)
        send_relay(W1)
        for r in (pieces,) + tuple(range(pieces)):
            cast_forward(TOK, r)
        pl.when(inner)(lambda: out_pass(0))
        for ch in (W0, W1):
            for d in range(nz):
                pass_theirs(ch, d)


    gain_copy.wait()

    def normalize(which):
        wide = tok[which].astype(jnp.float32)
        normed[at_multiple(which * rows, rows, rows), :] = (
            wide * lax.rsqrt(jnp.mean(wide * wide, axis=-1, keepdims=True) + EPS) * gain[...]
        ).astype(jnp.bfloat16)

    normalize(x)

    q_rows, span = 2 * SEG, (LEFT + 2) * SEG
    heads = half_cols // HEAD_DIM
    blocks = 2 * rows // q_rows

    pl.when(jnp.logical_not(first_entry))(lambda: line_copy(0).wait_recv())
    q_seg = lax.broadcasted_iota(jnp.int32, (q_rows, span), 0) // SEG
    k_seg = lax.broadcasted_iota(jnp.int32, (q_rows, span), 1) // SEG
    near = (k_seg >= q_seg) & (k_seg <= q_seg + LEFT)
    length = table.shape[1]
    line_len = (LEFT + 4) * SEG
    entry_of = lax.broadcasted_iota(jnp.int32, (length, line_len), 0)
    back = LEFT * SEG - lax.broadcasted_iota(jnp.int32, (length, line_len), 1)
    back = jnp.where(back < -REL_CLIP, REL_CLIP, jnp.minimum(back, REL_CLIP))
    pick = (entry_of == back + REL_CLIP).astype(jnp.float32)
    lines = jnp.dot(table[...], pick, precision=lax.Precision.HIGHEST, preferred_element_type=jnp.float32)
    lines = jnp.where(x == 0, lines[:heads], lines[heads:])
    for h in range(heads):
        line = jnp.broadcast_to(lines[h : h + 1, :], (q_rows, line_len))
        skew = pltpu.roll(line, 0, 1, stride=1, stride_axis=0)
        bias[h] = jnp.where(near, skew[:, :span], NEG)

    for r in range(pieces + 1):
        across_in(TOK, r).wait_recv()
    normalize(1 - x)
    pl.when(has_next)(lambda: halo(pairs).start())

    def project(p):
        made = jnp.dot(normed[...], w_all[p], preferred_element_type=jnp.float32).astype(jnp.bfloat16)
        kv_all[p, pl.ds(rows, 2 * rows), :] = made[:, : 2 * lanes]
        q_buf[p] = (made[:, 2 * lanes :].astype(jnp.float32) * HEAD_DIM ** (-0.5)).astype(jnp.bfloat16)
        pl.when(has_next)(lambda: halo(p).start())

    middle = jnp.logical_not(entry) & inner
    late = jnp.logical_not(second_entry) & outer
    project(0)
    pl.when(middle)(lambda: out_pass(1))
    project(1)

    @pl.when(middle)
    def _():
        out_pass(2)
        out_pass(3)

    @pl.when(second_entry & inner)
    def _():
        for r in range(n_tp):
            out_near(r)

    @pl.when(first_entry & inner)
    def _():
        for r in range(n_tp // 2, n_tp):
            wo_aid_copy(r).wait()
            wo_aid_send_on(r).start()

    low = lax.broadcasted_iota(jnp.int32, (q_rows, lanes), 1) < HEAD_DIM
    eye = lax.broadcasted_iota(jnp.int32, (q_rows, q_rows), 0) == lax.broadcasted_iota(jnp.int32, (q_rows, q_rows), 1)

    def make_mask(j):
        q_docs = docs_all[pl.ds(0, 1), pl.ds(rows + j * q_rows, q_rows)].astype(jnp.float32)
        k_docs = docs_all[pl.ds(0, 1), pl.ds(j * q_rows, span)].astype(jnp.float32)
        column = jnp.sum(jnp.where(eye, jnp.broadcast_to(q_docs, (q_rows, q_rows)), 0.0), axis=1, keepdims=True)
        mask[j] = jnp.where(column == k_docs, 0.0, NEG)

    def attend_rows(p, j):
        keys = pl.ds(j * q_rows, span)
        q_pair = q_buf[p, pl.ds(j * q_rows, q_rows), :]
        k_pair = kv_all[p, keys, pl.ds(0, lanes)]
        v_pair = kv_all[p, keys, pl.ds(lanes, lanes)]
        both = []
        for half in range(2):
            on = low if half == 0 else jnp.logical_not(low)
            q_one = jnp.where(on, q_pair, jnp.zeros_like(q_pair))
            score = lax.dot_general(q_one, k_pair, (((1,), (1,)), ((), ())), preferred_element_type=jnp.float32)
            score = score + bias[2 * p + half] + mask[j]
            raised = jnp.exp(score - jnp.max(score, axis=-1, keepdims=True))
            total = jnp.sum(raised, axis=-1, keepdims=True)
            both.append(jnp.dot(raised.astype(jnp.bfloat16), v_pair, preferred_element_type=jnp.float32) / total)
        return jnp.where(low, both[0], both[1]).astype(jnp.bfloat16)

    per = blocks // 2

    def attend_half(p, which):
        for j in range(per):
            found = attend_rows(p, which * per + j)
            part = pl.ds(j * q_rows, q_rows)
            att_own[p, which, part, :] = found

            @pl.when(first_entry & (x == which))
            def _():
                att_all[t, part, at_multiple(x * half_cols + p * lanes, lanes, lanes)] = found

        pl.when(x == which)(lambda: send_direct(A0 + p))
        pl.when(x != which)(lambda: send_cross(A0 + p))

    for j in range(per, blocks):
        make_mask(j)
    attend_half(0, 1)

    @pl.when(has_prev)
    def _():
        for i in (pairs, 0):
            halo(i).wait_recv()

    for j in range(per):
        make_mask(j)
    attend_half(0, 0)
    pl.when(late)(lambda: out_pass(0))
    pl.when(jnp.logical_not(second_entry))(lambda: out_across(0))
    attend_half(1, 1)
    send_relay(A0)
    pl.when(has_prev)(lambda: halo(1).wait_recv())
    attend_half(1, 0)
    pl.when(late)(lambda: out_pass(1))
    out_across(1)
    send_relay(A1)
    pl.when(late)(lambda: out_pass(2))
    out_across(2)
    pl.when(late)(lambda: out_pass(3))
    out_across(3)

    for ch in (A0, A1):
        for d in range(nz):
            pass_mine(ch, d)
    for ch in (A0, A1):
        for d in range(nz):
            pass_theirs(ch, d)

    half_chunk = chunk // 2

    def store(which, i):
        return pltpu.make_async_copy(
            done.at[which, i], out_ref.at[:, at_multiple(which * chunk + i * half_chunk, half_chunk, half_chunk)],
            store_sem.at[which, i],
        )

    def tp_move(way, i):
        which, target = ((home_y, t_y), (home_y, t_core), (home, t_core))[way]
        ref = done.at[which, i]
        return remote(ref, ref, tp_send.at[way, i], tp_recv.at[way, i], tp=target)

    def out_project(i):
        made = jnp.zeros((rows, half_chunk), jnp.float32)
        for r in range(n_tp):
            made = made + jnp.dot(att_all[r], wo_all[2 * r + i], preferred_element_type=jnp.float32)
        part = at_multiple(i * half_chunk, half_chunk, half_chunk)
        done[home_y, i] = (resid[:, part].astype(jnp.float32) + made).astype(jnp.bfloat16)
        tp_move(0, i).start()
        tp_move(1, i).start()
        store(home_y, i).start()

    resid_copy.wait()
    out_project(x)
    for r in range(n_tp):
        across_in(OUT, r).wait_recv()
    out_project(1 - x)
    for i in (x, 1 - x):
        tp_move(0, i).wait_recv()
        tp_move(2, i).start()
        store(home, i).start()
    for i in (x, 1 - x):
        tp_move(1, i).wait_recv()
        store(plane_of(t_far), i).start()
    for i in (x, 1 - x):
        tp_move(2, i).wait_recv()
        store(plane_of(t_core), i).start()
    for which in range(n_tp):
        for i in range(2):
            store(which, i).wait()

    for ch in range(4):
        drain(ch)
    cast_drain(TOK, pieces + 1)
    cast_drain(OUT, n_tp)

    @pl.when(second_entry & inner)
    def _():
        for r in range(pieces // 2, pieces):
            aid_send_on(r).wait_send()

    @pl.when(first_entry & inner)
    def _():
        for r in range(n_tp // 2, n_tp):
            wo_aid_send_on(r).wait_send()

    @pl.when(first_entry)
    def _():
        for i in range(3):
            line_copy(i).wait_send()

    @pl.when(has_next)
    def _():
        for i in range(pairs + 1):
            halo(i).wait_send()
    for way in range(3):
        for i in range(2):
            tp_move(way, i).wait_send()


def body_one(n_sp, n_tp, tokens, documents, norm_gain, w_query, w_key, w_value, w_out, rel_bias):
    rows, width = tokens.shape
    depth, cols = w_query.shape[1:]
    heads = cols // HEAD_DIM
    out_cols = w_out.shape[2]
    chunk = width // n_tp
    lanes = 2 * HEAD_DIM
    pairs = cols // 2 // lanes
    table = rel_bias[0]
    bf, f32 = jnp.bfloat16, jnp.float32
    hbm = pl.BlockSpec(memory_space=pl.ANY)
    dma = pltpu.SemaphoreType.DMA
    q_rows, span = 2 * SEG, (LEFT + 2) * SEG
    return pl.pallas_call(
        functools.partial(layer_kernel, n_sp, n_tp),
        out_shape=jax.ShapeDtypeStruct((rows, width), bf),
        in_specs=[hbm] * 8,
        out_specs=hbm,
        scratch_shapes=[
            pltpu.VMEM((2, pairs, depth, 3 * lanes), bf),
            pltpu.VMEM((pairs, depth, 3 * lanes), bf),
            pltpu.VMEM((pairs, n_sp * depth, 3 * lanes), bf),
            pltpu.VMEM((n_sp, cols, out_cols), bf),
            pltpu.VMEM((2, rows, width), bf),
            pltpu.VMEM((rows // 2, width), bf),
            pltpu.VMEM((n_tp // 2, cols, out_cols), bf),
            pltpu.VMEM((rows, chunk), bf),
            pltpu.VMEM((2 * rows, width), bf),
            pltpu.VMEM((1, width), f32),
            pltpu.VMEM(table.shape, f32),
            pltpu.VMEM((heads // 2, q_rows, span), f32),
            pltpu.VMEM((pairs, 2 * rows, lanes), bf),
            pltpu.VMEM((pairs, 3 * rows, 2 * lanes), bf),
            pltpu.VMEM((1, 3 * rows), jnp.int32),
            pltpu.VMEM((2 * rows // q_rows, q_rows, span), f32),
            pltpu.VMEM((pairs, 2, rows, lanes), bf),
            pltpu.VMEM((pairs, rows, lanes), bf),
            pltpu.VMEM((n_tp, rows, cols), bf),
            pltpu.VMEM((n_tp, 2, rows, chunk // 2), bf),
            dma((2, pairs, 3)),
            dma((pairs, 3)),
            dma((n_tp,)),
            dma((n_tp,)),
            dma(()),
            dma((n_tp // 2,)),
            dma((n_tp // 2,)),
            dma((n_tp // 2,)),
            dma(()),
            dma((3,)),
            dma((3,)),
            dma(()),
            dma((4, 3)),
            dma((4,)),
            dma((4, 2, n_sp)),
            dma((4, n_sp)),
            dma((2, 3, n_tp + 1)),
            dma((2, 2, n_tp + 1)),
            dma((pairs + 1,)),
            dma((pairs + 1,)),
            dma((3, 2)),
            dma((3, 2)),
            dma((n_tp, 2)),
        ],
        compiler_params=pltpu.CompilerParams(
            collective_id=0, has_side_effects=True, vmem_limit_bytes=60 * 1024 * 1024
        ),
    )(documents[None, :], norm_gain, table, tokens, w_key[0], w_value[0], w_query[0], w_out[0])


def fits_one(mesh):
    return mesh.shape["tp"] == 4 and mesh.shape["sp"] == 2 * mesh.shape["tp"]


def solution(mesh):
    n_sp, n_tp = mesh.shape["sp"], mesh.shape["tp"]
    run = functools.partial(body_one, n_sp, n_tp) if fits_one(mesh) else body
    in_specs = (
        P("sp", None),
        P("sp"),
        P(),
        P(None, "sp", "tp"),
        P(None, "sp", "tp"),
        P(None, "sp", "tp"),
        P(None, None, "sp"),
        P(None, "tp", None),
    )
    out_specs = P("sp", None)
    return jax.shard_map(run, mesh=mesh, in_specs=in_specs, out_specs=out_specs, check_vma=False)
```

```python
import functools

import jax
import jax.numpy as jnp
from jax import lax
from jax.experimental import pallas as pl
from jax.experimental.pallas import tpu as pltpu
from jax.sharding import PartitionSpec as P

HEAD_DIM = 64
SEG = 64
LEFT = 4
REL_CLIP = 128


EPS = 1e-06


def passed_along(x, axis, by):
    length = lax.axis_size(axis)
    pairs = [(i, i + by) for i in range(length) if 0 <= i + by < length]
    return lax.ppermute(x, axis, pairs)


def banded_bias(bias_table, query_rows, key_rows, reach_rows):
    span_len = query_rows + key_rows - 1
    steps_back = jnp.arange(span_len, dtype=jnp.int32) - (key_rows - 1) + reach_rows
    lookup = jnp.clip(steps_back, -REL_CLIP, REL_CLIP) + REL_CLIP
    bias_line = jnp.take(bias_table, lookup, axis=1)
    reversed_line = bias_line[:, ::-1]
    repeated = jnp.tile(reversed_line, (1, query_rows))
    skewed = repeated[:, query_rows - 1 : query_rows - 1 + query_rows * (span_len - 1)]
    skewed = skewed.reshape(bias_table.shape[0], query_rows, span_len - 1)
    return skewed[:, :, :key_rows]


def attend(queries, keys_all, values_all, query_pos, key_pos, query_doc, key_doc, bias_table):
    query_rows = queries.shape[0]
    key_rows = keys_all.shape[0]
    reach_rows = key_rows - query_rows
    scores = jnp.einsum(
        "qhe,khe->hqk", queries, keys_all, preferred_element_type=jnp.float32
    ) * HEAD_DIM ** (-0.5)
    scores = scores + banded_bias(bias_table, query_rows, key_rows, reach_rows)
    query_seg = query_pos // SEG
    key_seg = key_pos // SEG
    allowed = (
        (key_pos[None, :] >= 0)
        & (key_seg[None, :] <= query_seg[:, None])
        & (key_seg[None, :] >= query_seg[:, None] - LEFT)
        & (key_doc[None, :] == query_doc[:, None])
    )
    scores = jnp.where(allowed[None], scores, -1e30)
    peak = jnp.max(scores, axis=-1, keepdims=True)
    raised = jnp.exp(scores - peak)
    weights_bf = (raised / jnp.sum(raised, axis=-1, keepdims=True)).astype(jnp.bfloat16)
    return jnp.einsum(
        "hqk,khe->qhe", weights_bf, values_all, preferred_element_type=jnp.float32
    ).astype(jnp.bfloat16)


def body(tokens, documents, norm_gain, w_query, w_key, w_value, w_out, rel_bias):
    local_rows = tokens.shape[0]
    reach_rows = LEFT * SEG
    width_local = w_query.shape[2]
    heads_local = width_local // HEAD_DIM
    offset = lax.axis_index("sp") * local_rows
    query_pos = offset + jnp.arange(local_rows, dtype=jnp.int32)
    key_pos = offset - reach_rows + jnp.arange(reach_rows + local_rows, dtype=jnp.int32)
    widened = tokens.astype(jnp.float32)
    normed = (
        widened
        * lax.rsqrt(jnp.mean(widened * widened, axis=-1, keepdims=True) + EPS)
        * norm_gain[0]
    ).astype(jnp.bfloat16)
    query_sum = jnp.dot(
        normed,
        lax.all_gather(w_query[0], "sp", axis=0, tiled=True),
        preferred_element_type=jnp.float32,
    )
    key_sum = jnp.dot(
        normed,
        lax.all_gather(w_key[0], "sp", axis=0, tiled=True),
        preferred_element_type=jnp.float32,
    )
    value_sum = jnp.dot(
        normed,
        lax.all_gather(w_value[0], "sp", axis=0, tiled=True),
        preferred_element_type=jnp.float32,
    )
    queries = query_sum.astype(jnp.bfloat16)
    keys_own = key_sum.astype(jnp.bfloat16)
    values_own = value_sum.astype(jnp.bfloat16)
    prior_keys, prior_values, prior_docs = passed_along((keys_own, values_own, documents), "sp", 1)
    keys_all = jnp.concatenate([prior_keys, keys_own], axis=0)
    values_all = jnp.concatenate([prior_values, values_own], axis=0)
    key_doc = jnp.concatenate([prior_docs, documents], axis=0)
    attended = attend(
        queries.reshape(local_rows, heads_local, HEAD_DIM),
        keys_all.reshape(reach_rows + local_rows, heads_local, HEAD_DIM),
        values_all.reshape(reach_rows + local_rows, heads_local, HEAD_DIM),
        query_pos,
        key_pos,
        documents,
        key_doc,
        rel_bias[0],
    ).reshape(local_rows, width_local)
    all_heads = lax.all_gather(attended, "tp", axis=1, tiled=True)
    return (
        widened
        + jnp.dot(
            all_heads,
            lax.all_gather(w_out[0], "sp", axis=1, tiled=True),
            preferred_element_type=jnp.float32,
        )
    ).astype(jnp.bfloat16)


MESH = pl.DeviceIdType.MESH
TOK, OUT = range(2)
UP, DOWN, ACROSS = range(3)
W0, W1, A0, A1 = range(4)
NEG = -1e30


def plane_of(t):
    c = t % 2
    return 3 * c + (t // 2) * (1 - 2 * c)


def part_for(z):
    return 2 * (((z + 1) // 2) % 2) + z // 2


def layer_kernel(
    n_sp, n_tp, doc_in, gain_in, table_in, x_in, wk_in, wv_in, wq_in, wo_in, out_ref,
    w_own, w_relay, w_all, wo_all, tok, aid, wo_aid, resid, normed, gain, table, bias, q_buf, kv_all, docs_all, mask,
    att_own, att_relay, att_all,
    own_sem, loc_sem, out_sem, tok_sem, aid_sem, aid_send, wo_aid_sem, wo_aid_send, res_sem, small_sem, line_send, line_recv, hop_send, relay_recv, rep_send, rep_recv,
    cast_send, cast_recv, halo_send, halo_recv, tp_send, tp_recv,
):
    rows, width = tok.shape[1:]
    depth, cols = wk_in.shape
    half_cols = cols // 2
    lanes = 2 * HEAD_DIM
    pairs = half_cols // lanes
    q_rows, span = 2 * SEG, (LEFT + 2) * SEG
    chunk = width // n_tp
    nz = n_sp // 2
    pieces = 2 * n_tp
    piece = rows // pieces
    s = lax.axis_index("sp")
    t = lax.axis_index("tp")
    z, x = s // 2, s % 2
    mate = s + 1 - 2 * x
    ty, tc = t // 2, t % 2
    t_core = t + 1 - 2 * tc
    t_y = (1 - ty) * 2 + tc
    t_far = (1 - ty) * 2 + 1 - tc
    home, home_y = plane_of(t), plane_of(t_y)
    first_entry, second_entry = z == home, z == home_y
    entry = first_entry | second_entry
    gap = z - home
    is_first = 1 - (gap * gap + n_sp) // (n_sp + 1)
    x_mine = x * is_first + (1 - x) * (1 - is_first)
    own_in = (wk_in, wv_in, wq_in)
    has_up, has_down = z < nz - 1, z > 0

    def at_multiple(start, size, step):
        return pl.ds(pl.multiple_of(start, step), size)

    def weight_cols(which, p):
        return at_multiple(which * half_cols + p * lanes, lanes, lanes)

    def kind_cols(kind):
        return pl.ds(kind * lanes, lanes)

    def own_copy(i, p, kind):
        which = x if i == 0 else 1 - x
        return pltpu.make_async_copy(
            own_in[kind].at[:, weight_cols(which, p)], w_own.at[i, p, :, kind_cols(kind)], own_sem.at[i, p, kind]
        )

    def local_copy(p, kind):
        return pltpu.make_async_copy(
            own_in[kind].at[:, weight_cols(x, p)],
            w_all.at[p, at_multiple(s * depth, depth, depth), kind_cols(kind)], loc_sem.at[p, kind],
        )

    def tok_copy(r):
        part = pl.ds(r * piece, piece)
        return pltpu.make_async_copy(x_in.at[part, :], tok.at[x, part, :], tok_sem.at[r])

    def out_copy(r):
        return pltpu.make_async_copy(wo_in.at[pl.ds(r * cols, cols), :], wo_all.at[2 * r + x], out_sem.at[r])

    doc_copy = pltpu.make_async_copy(doc_in, docs_all.at[:, at_multiple((1 + x) * rows, rows, rows)], small_sem.at[0])
    gain_copy = pltpu.make_async_copy(gain_in, gain, small_sem.at[1])
    table_copy = pltpu.make_async_copy(table_in, table, small_sem.at[2])
    resid_copy = pltpu.make_async_copy(x_in.at[:, at_multiple(home_y * chunk, chunk, chunk)], resid, res_sem)

    gain_copy.start()

    @pl.when(first_entry)
    def _():
        doc_copy.start()
        for r in range(pieces):
            tok_copy(r).start()
        table_copy.start()

    for p in range(pairs):
        for i in (1, 0):
            for kind in range(3):
                own_copy(i, p, kind).start()

    @pl.when(first_entry)
    def _():
        for p in range(pairs):
            for kind in range(3):
                local_copy(p, kind).start()

    outer = (z == 0) | (z == nz - 1)
    inner = jnp.logical_not(outer)
    lower = z < nz // 2
    aid_copy = pltpu.make_async_copy(x_in.at[pl.ds(rows - 4 * piece, 4 * piece), :], aid, aid_sem)

    def wo_aid_copy(r):
        return pltpu.make_async_copy(wo_in.at[pl.ds(r * cols, cols), :], wo_aid.at[r - 1], wo_aid_sem.at[r - 1])

    aide = inner & (z == plane_of(t_far))

    @pl.when(aide)
    def _():
        for r in range(1, n_tp):
            wo_aid_copy(r).start()

    @pl.when(second_entry)
    def _():
        pl.when(inner)(lambda: aid_copy.start())

        for r in range(n_tp):
            out_copy(r).start()

    resid_copy.start()

    def remote(src, dst, send, recv, **where):
        return pltpu.make_async_remote_copy(
            src_ref=src, dst_ref=dst, send_sem=send, recv_sem=recv, device_id=where, device_id_type=MESH
        )

    def slot(ch, block):
        if ch < A0:
            return w_all.at[ch - W0, at_multiple(block * depth, depth, depth), :]
        return att_all.at[
            part_for(block // 2), pl.ds((ch - A0) * q_rows, q_rows), at_multiple((block % 2) * half_cols, half_cols, half_cols)
        ]

    def own_ref(ch, i):
        return w_own.at[i, ch - W0] if ch < A0 else att_own.at[ch - A0, x if i == 0 else 1 - x]

    def relay_ref(ch):
        return w_relay.at[ch - W0] if ch < A0 else att_relay.at[ch - A0]

    def direct(ch):
        return remote(own_ref(ch, 0), slot(ch, s), hop_send.at[ch, 0], rep_recv.at[ch, s], sp=2 * home + x)

    def cross_in(ch):
        return remote(own_ref(ch, 1), slot(ch, s), hop_send.at[ch, 1], rep_recv.at[ch, s], sp=mate, tp=t_y)

    def cross_relay(ch):
        return remote(own_ref(ch, 1), relay_ref(ch), hop_send.at[ch, 1], relay_recv.at[ch], sp=mate, tp=t_y)

    def relay(ch):
        return remote(relay_ref(ch), slot(ch, mate), hop_send.at[ch, 2], rep_recv.at[ch, mate], sp=2 * home_y + x)

    def to_y(ch, block):
        return remote(slot(ch, block), slot(ch, block), rep_send.at[ch, 0, block], rep_recv.at[ch, block], tp=t_y)

    def to_core(ch, block):
        return remote(slot(ch, block), slot(ch, block), rep_send.at[ch, 1, block], rep_recv.at[ch, block], tp=t_core)

    def send_cross(ch):
        pl.when(first_entry)(lambda: cross_in(ch).start())
        pl.when(jnp.logical_not(first_entry))(lambda: cross_relay(ch).start())

    def send_direct(ch):
        pl.when(jnp.logical_not(first_entry))(lambda: direct(ch).start())

    def send_relay(ch):
        @pl.when(jnp.logical_not(second_entry))
        def _():
            cross_relay(ch).wait_recv()
            relay(ch).start()

    planes = [0]
    for d in range(1, nz):
        planes += [-d, d]

    def valid(off):
        return (z + off >= 0) & (z + off < nz)

    def mine(ch, off):
        @pl.when(entry & valid(off))
        def _():
            block = 2 * (z + off) + x_mine
            if off == 0:
                pl.when(jnp.logical_not(first_entry))(lambda: to_y(ch, block).wait_recv())
                if ch < A0:
                    @pl.when(first_entry)
                    def _():
                        for kind in range(3):
                            local_copy(ch - W0, kind).wait()
            else:
                to_y(ch, block).wait_recv()
            to_y(ch, block).start()
            to_core(ch, block).start()

    def theirs(ch, off):
        @pl.when(valid(off))
        def _():
            @pl.when(entry)
            def _():
                block = 2 * (z + off) + 1 - x_mine
                to_y(ch, block).wait_recv()
                to_core(ch, block).start()

            @pl.when(jnp.logical_not(entry))
            def _():
                for i in range(2):
                    to_core(ch, 2 * (z + off) + i).wait_recv()

    def spread(ch, first, last):
        for i in range(first, last + 1):
            if i < len(planes):
                mine(ch, planes[i])
            if i > 0:
                theirs(ch, planes[i - 1])

    def drain(ch):
        pl.when(jnp.logical_not(first_entry))(lambda: direct(ch).wait_send())
        cross_relay(ch).wait_send()
        pl.when(jnp.logical_not(second_entry))(lambda: relay(ch).wait_send())

        @pl.when(entry)
        def _():
            for zz in range(nz):
                to_y(ch, 2 * zz + x_mine).wait_send()
                for i in range(2):
                    to_core(ch, 2 * zz + i).wait_send()

    def cast_ref(kind, which, r):
        if kind == OUT:
            return wo_all.at[2 * r + which]
        if r == pieces:
            return docs_all.at[:, at_multiple((1 + which) * rows, rows, rows)]
        return tok.at[which, pl.ds(r * piece, piece), :]

    def move(kind, way, r, src=None):
        ref = cast_ref(kind, x, r)
        return remote(
            ref if src is None else src, ref, cast_send.at[kind, way, r], cast_recv.at[kind, x, r],
            sp=(s + 2, s - 2, mate)[way],
        )

    def across_in(kind, r):
        ref = cast_ref(kind, 1 - x, r)
        return remote(ref, ref, cast_send.at[kind, ACROSS, r], cast_recv.at[kind, 1 - x, r], sp=mate)

    centers = (home, home_y)

    def aided(kind, r):
        return pieces - 4 <= r < pieces if kind == TOK else r > 0

    def goes(kind, way, r):
        ok = (z >= centers[kind]) & has_up if way == UP else (z <= centers[kind]) & has_down
        if aided(kind, r):
            near = jnp.logical_not(lower) if way == UP else lower
            ok = ok & jnp.logical_not((z == centers[kind]) & inner & near)
        return ok

    def aid_move(i):
        r = pieces - 4 + i
        return remote(
            aid.at[pl.ds(i * piece, piece), :], cast_ref(TOK, x, r), aid_send.at[i], cast_recv.at[TOK, x, r],
            sp=s + 2 - 4 * (1 - z // (nz // 2)), tp=t_y,
        )

    def wo_aid_move(r):
        return remote(
            wo_aid.at[r - 1], cast_ref(OUT, x, r), wo_aid_send.at[r - 1], cast_recv.at[OUT, x, r],
            sp=s + 2 - 4 * (1 - z // (nz // 2)), tp=t_core,
        )

    def cast_along(kind, r, src=None):
        for way in (UP, DOWN):
            pl.when(goes(kind, way, r))(lambda: move(kind, way, r, src).start())

    def cast_send_on(kind, r, src=None):
        cast_along(kind, r, src)
        move(kind, ACROSS, r, src).start()

    def cast_source(kind, r):
        if r == pieces and kind == TOK:
            doc_copy.wait()
            cast_send_on(kind, r)
            return
        (tok_copy, out_copy)[kind](r).wait()
        cast_send_on(kind, r)

    def cast_forward(kind, r):
        @pl.when(z != centers[kind])
        def _():
            move(kind, UP, r).wait_recv()
            cast_send_on(kind, r)

    def cast_drain(kind, count):
        for r in range(count):
            for way in (UP, DOWN):
                pl.when(goes(kind, way, r))(lambda: move(kind, way, r).wait_send())
            move(kind, ACROSS, r).wait_send()

    line_targets = (t_core, t_y, t_far)

    def line_copy(i):
        return remote(table, table, line_send.at[i], line_recv, tp=line_targets[i])

    has_next, has_prev = home < nz - 1, home > 0

    def halo(i):
        if i == pairs:
            src, dst = docs_all.at[:, pl.ds(2 * rows, rows)], docs_all.at[:, pl.ds(0, rows)]
        else:
            src, dst = kv_all.at[i, pl.ds(2 * rows, rows), :], kv_all.at[i, pl.ds(0, rows), :]
        return remote(src, dst, halo_send.at[i], halo_recv.at[i], tp=part_for((home + 1) % nz))

    barrier = pltpu.get_barrier_semaphore()
    for d in range(1, nz):
        pl.semaphore_signal(
            barrier, inc=1, device_id={"sp": lax.rem(s + 2 * d, n_sp)}, device_id_type=MESH
        )
    for peer in (t_core, t_y, t_far):
        pl.semaphore_signal(barrier, inc=1, device_id={"tp": peer}, device_id_type=MESH)
    for peer in (t, t_y):
        pl.semaphore_signal(barrier, inc=1, device_id={"sp": mate, "tp": peer}, device_id_type=MESH)
    pl.semaphore_signal(
        barrier, inc=1, device_id={"sp": s + 2 - 4 * (z % 2), "tp": t_y}, device_id_type=MESH
    )
    pl.semaphore_signal(
        barrier, inc=1, device_id={"sp": s + 2 - 4 * (z % 2), "tp": t_core}, device_id_type=MESH
    )
    pl.semaphore_wait(barrier, nz + 6)

    for p in range(pairs):
        for i in (1, 0):
            for kind in range(3):
                own_copy(i, p, kind).wait()
            (send_direct, send_cross)[i](W0 + p)

    @pl.when(first_entry)
    def _():
        for r in (pieces,) + tuple(range(pieces)):
            cast_source(TOK, r)
        table_copy.wait()
        for i in range(3):
            line_copy(i).start()

    def out_along(r):
        out_copy(r).wait()
        cast_along(OUT, r)

    def out_near(r):
        pl.when(goes(OUT, UP, r) & jnp.logical_not(lower))(lambda: move(OUT, UP, r).start())
        pl.when(goes(OUT, DOWN, r) & lower)(lambda: move(OUT, DOWN, r).start())

    def out_far(r):
        pl.when(goes(OUT, UP, r) & lower)(lambda: move(OUT, UP, r).start())
        pl.when(goes(OUT, DOWN, r) & jnp.logical_not(lower))(lambda: move(OUT, DOWN, r).start())

    def out_across(r):
        move(OUT, ACROSS, r).start()

    def out_pass(r):
        @pl.when(z != home_y)
        def _():
            move(OUT, UP, r).wait_recv()
            cast_along(OUT, r)

    @pl.when(second_entry)
    def _():
        @pl.when(inner)
        def _():
            aid_copy.wait()
            for i in range(4):
                aid_move(i).start()

        @pl.when(outer)
        def _():
            for r in range(n_tp):
                out_along(r)

    @pl.when(has_prev == False)
    def _():
        docs_all[:, pl.ds(0, rows)] = jnp.full((1, rows), -1, jnp.int32)
        for p in range(pairs):
            kv_all[p, pl.ds(0, rows), :] = jnp.zeros((rows, 2 * lanes), jnp.bfloat16)

    def around(d):
        return (0,) if d == 0 else (-d, d)

    def pass_mine(ch, d):
        for off in around(d):
            mine(ch, off)

    def pass_theirs(ch, d):
        for off in around(d):
            theirs(ch, off)

    @pl.when(first_entry)
    def _():
        pass_mine(W0, 0)
        pass_mine(W1, 0)
        send_relay(W0)
        send_relay(W1)
        for ch in (W0, W1):
            for d in range(1, nz):
                pass_mine(ch, d)

        @pl.when(inner)
        def _():
            for r in range(n_tp):
                out_pass(r)
                if r < 2:
                    out_across(r)

        @pl.when(outer)
        def _():
            out_pass(0)
            out_across(0)

        for ch in (W0, W1):
            for d in range(nz):
                pass_theirs(ch, d)

    @pl.when(second_entry)
    def _():
        pass_mine(W0, 0)
        cast_forward(TOK, pieces)
        for r in range(0, 2):
            cast_forward(TOK, r)

        @pl.when(inner)
        def _():
            out_copy(0).wait()
            out_near(0)

        out_across(0)
        pass_mine(W1, 0)
        for r in range(2, 4):
            cast_forward(TOK, r)
        pl.when(inner)(lambda: out_copy(1).wait())
        out_across(1)
        pass_mine(W0, 1)
        pass_mine(W1, 1)
        for r in range(4, 6):
            cast_forward(TOK, r)
        pass_mine(W0, 2)
        pass_mine(W1, 2)
        for r in range(6, 8):
            cast_forward(TOK, r)
        pass_mine(W0, 3)
        pass_mine(W1, 3)

        @pl.when(inner)
        def _():
            for r in range(n_tp):
                if r >= 2:
                    out_copy(r).wait()
                out_far(r)

        for ch in (W0, W1):
            for d in range(nz):
                pass_theirs(ch, d)

    @pl.when(jnp.logical_not(entry))
    def _():
        send_relay(W0)
        send_relay(W1)
        for r in (pieces,) + tuple(range(pieces)):
            cast_forward(TOK, r)

        @pl.when(aide)
        def _():
            for r in range(1, n_tp):
                wo_aid_copy(r).wait()
                wo_aid_move(r).start()

        pl.when(inner)(lambda: out_pass(0))
        for ch in (W0, W1):
            for d in range(nz):
                pass_theirs(ch, d)


    gain_copy.wait()

    def normalize(which):
        wide = tok[which].astype(jnp.float32)
        normed[at_multiple(which * rows, rows, rows), :] = (
            wide * lax.rsqrt(jnp.mean(wide * wide, axis=-1, keepdims=True) + EPS) * gain[...]
        ).astype(jnp.bfloat16)

    normalize(x)

    heads = half_cols // HEAD_DIM
    blocks = 2 * rows // q_rows

    pl.when(jnp.logical_not(first_entry))(lambda: line_copy(0).wait_recv())
    q_seg = lax.broadcasted_iota(jnp.int32, (q_rows, span), 0) // SEG
    k_seg = lax.broadcasted_iota(jnp.int32, (q_rows, span), 1) // SEG
    near = (k_seg >= q_seg) & (k_seg <= q_seg + LEFT)
    length = table.shape[1]
    line_len = (LEFT + 4) * SEG
    entry_of = lax.broadcasted_iota(jnp.int32, (length, line_len), 0)
    back = LEFT * SEG - lax.broadcasted_iota(jnp.int32, (length, line_len), 1)
    back = jnp.where(back < -REL_CLIP, REL_CLIP, jnp.minimum(back, REL_CLIP))
    pick = (entry_of == back + REL_CLIP).astype(jnp.float32)
    lines = jnp.dot(table[...], pick, precision=lax.Precision.HIGHEST, preferred_element_type=jnp.float32)
    lines = jnp.where(x == 0, lines[:heads], lines[heads:])
    for h in range(heads):
        line = jnp.broadcast_to(lines[h : h + 1, :], (q_rows, line_len))
        skew = pltpu.roll(line, 0, 1, stride=1, stride_axis=0)
        bias[h] = jnp.where(near, skew[:, :span], NEG)

    def project(which):
        own = at_multiple(which * rows, rows, rows)
        for p in range(pairs):
            made = jnp.dot(normed[own, :], w_all[p], preferred_element_type=jnp.float32).astype(jnp.bfloat16)
            kv_all[p, at_multiple((1 + which) * rows, rows, rows), :] = made[:, : 2 * lanes]
            q_buf[p, own, :] = (made[:, 2 * lanes :].astype(jnp.float32) * HEAD_DIM ** (-0.5)).astype(jnp.bfloat16)

    def send_halo():
        for p in range(pairs):
            halo(p).start()

    project(x)
    pl.when(has_next & (x == 1))(send_halo)
    middle = jnp.logical_not(entry) & inner

    pl.when(middle)(lambda: out_pass(1))
    for r in range(pieces + 1):
        across_in(TOK, r).wait_recv()
    pl.when(has_next)(lambda: halo(pairs).start())
    normalize(1 - x)
    late = jnp.logical_not(second_entry) & outer
    project(1 - x)
    pl.when(has_next & (x == 0))(send_halo)

    low = lax.broadcasted_iota(jnp.int32, (q_rows, lanes), 1) < HEAD_DIM
    eye = lax.broadcasted_iota(jnp.int32, (q_rows, q_rows), 0) == lax.broadcasted_iota(jnp.int32, (q_rows, q_rows), 1)

    def make_mask(j):
        q_docs = docs_all[pl.ds(0, 1), pl.ds(rows + j * q_rows, q_rows)].astype(jnp.float32)
        k_docs = docs_all[pl.ds(0, 1), pl.ds(j * q_rows, span)].astype(jnp.float32)
        column = jnp.sum(jnp.where(eye, jnp.broadcast_to(q_docs, (q_rows, q_rows)), 0.0), axis=1, keepdims=True)
        mask[j] = jnp.where(column == k_docs, 0.0, NEG)

    def attend_rows(g):
        keys, queries = pl.ds(g * q_rows, span), pl.ds(g * q_rows, q_rows)
        found = []
        for p in range(pairs):
            q_pair = q_buf[p, queries, :]
            k_pair = kv_all[p, keys, pl.ds(0, lanes)]
            v_pair = kv_all[p, keys, pl.ds(lanes, lanes)]
            both = []
            for half in range(2):
                on = low if half == 0 else jnp.logical_not(low)
                q_one = jnp.where(on, q_pair, jnp.zeros_like(q_pair))
                score = lax.dot_general(q_one, k_pair, (((1,), (1,)), ((), ())), preferred_element_type=jnp.float32)
                score = score + bias[2 * p + half] + mask[g]
                raised = jnp.exp(score - jnp.max(score, axis=-1, keepdims=True))
                total = jnp.sum(raised, axis=-1, keepdims=True)
                both.append(jnp.dot(raised.astype(jnp.bfloat16), v_pair, preferred_element_type=jnp.float32) / total)
            found.append(jnp.where(low, both[0], both[1]).astype(jnp.bfloat16))
        return jnp.concatenate(found, axis=1)

    per = blocks // 2

    def attend_step(j, which):
        found = attend_rows(which * per + j)
        att_own[j, which] = found

        @pl.when(first_entry & (x == which))
        def _():
            att_all[t, pl.ds(j * q_rows, q_rows), at_multiple(x * half_cols, half_cols, half_cols)] = found

        pl.when(x == which)(lambda: send_direct(A0 + j))
        pl.when(x != which)(lambda: send_cross(A0 + j))

    for g in range(per, blocks):
        make_mask(g)
    attend_step(0, 1)
    pl.when(middle)(lambda: out_pass(2))
    attend_step(1, 1)
    pl.when(middle)(lambda: out_pass(3))

    @pl.when(has_prev)
    def _():
        for i in (pairs,) + tuple(range(pairs)):
            halo(i).wait_recv()

    for g in range(per):
        make_mask(g)
    attend_step(0, 0)
    attend_step(1, 0)
    third = jnp.logical_not(entry)
    pl.when(third & outer)(lambda: out_pass(0))
    pl.when(third)(lambda: out_across(0))
    pl.when(first_entry & outer)(lambda: out_pass(1))
    pl.when(first_entry & outer)(lambda: out_across(1))
    send_relay(A0)
    send_relay(A1)
    pl.when(third & outer)(lambda: out_pass(1))
    pl.when(third)(lambda: out_across(1))
    swift = jnp.logical_not(late)

    @pl.when(swift)
    def _():
        out_across(2)
        out_across(3)

    for d in range(nz):
        for ch in (A0, A1):
            pass_mine(ch, d)

    @pl.when(late)
    def _():
        for r in (2, 3):
            out_pass(r)
            out_across(r)

    half_chunk = chunk // 2

    def result(which, j, i):
        cut = at_multiple(which * chunk + i * half_chunk, half_chunk, half_chunk)
        return out_ref.at[pl.ds(j * q_rows, q_rows), cut]

    def tp_move(way, j, i):
        which, target = ((home_y, t_y), (home_y, t_core), (home, t_core))[way]
        ref = result(which, j, i)
        return remote(ref, ref, tp_send.at[way, j, i], tp_recv.at[way, j, i], tp=target)

    def out_project(j, i):
        part = pl.ds(j * q_rows, q_rows)
        made = jnp.zeros((q_rows, half_chunk), jnp.float32)
        for r in range(n_tp):
            made = made + jnp.dot(att_all[r, part, :], wo_all[2 * r + i], preferred_element_type=jnp.float32)
        rest = resid[part, at_multiple(i * half_chunk, half_chunk, half_chunk)].astype(jnp.float32)
        result(home_y, j, i)[...] = (rest + made).astype(jnp.bfloat16)
        tp_move(0, j, i).start()
        tp_move(1, j, i).start()

    resid_copy.wait()
    for j in range(per):
        for d in range(nz):
            pass_theirs(A0 + j, d)
        out_project(j, x)
    for r in range(n_tp):
        across_in(OUT, r).wait_recv()
    for j in range(per):
        out_project(j, 1 - x)
    quarters = [(j, i) for i in (x, 1 - x) for j in range(per)]
    for q in quarters:
        tp_move(0, *q).wait_recv()
        tp_move(2, *q).start()
    for q in quarters:
        tp_move(1, *q).wait_recv()
        tp_move(2, *q).wait_recv()

    for ch in range(4):
        drain(ch)
    cast_drain(TOK, pieces + 1)
    cast_drain(OUT, n_tp)

    @pl.when(second_entry & inner)
    def _():
        for i in range(4):
            aid_move(i).wait_send()

    @pl.when(aide)
    def _():
        for r in range(1, n_tp):
            wo_aid_move(r).wait_send()


    @pl.when(first_entry)
    def _():
        for i in range(3):
            line_copy(i).wait_send()

    @pl.when(has_next)
    def _():
        for i in range(pairs + 1):
            halo(i).wait_send()
    for way in range(3):
        for q in quarters:
            tp_move(way, *q).wait_send()


def body_one(n_sp, n_tp, tokens, documents, norm_gain, w_query, w_key, w_value, w_out, rel_bias):
    rows, width = tokens.shape
    depth, cols = w_query.shape[1:]
    heads = cols // HEAD_DIM
    out_cols = w_out.shape[2]
    chunk = width // n_tp
    lanes = 2 * HEAD_DIM
    pairs = cols // 2 // lanes
    table = rel_bias[0]
    bf, f32 = jnp.bfloat16, jnp.float32
    hbm = pl.BlockSpec(memory_space=pl.ANY)
    dma = pltpu.SemaphoreType.DMA
    q_rows, span = 2 * SEG, (LEFT + 2) * SEG
    return pl.pallas_call(
        functools.partial(layer_kernel, n_sp, n_tp),
        out_shape=pltpu.VMEM((rows, width), bf),
        in_specs=[hbm] * 8,
        out_specs=pl.BlockSpec(memory_space=pltpu.VMEM),
        scratch_shapes=[
            pltpu.VMEM((2, pairs, depth, 3 * lanes), bf),
            pltpu.VMEM((pairs, depth, 3 * lanes), bf),
            pltpu.VMEM((pairs, n_sp * depth, 3 * lanes), bf),
            pltpu.VMEM((n_sp, cols, out_cols), bf),
            pltpu.VMEM((2, rows, width), bf),
            pltpu.VMEM((4 * rows // (2 * n_tp), width), bf),
            pltpu.VMEM((n_tp - 1, cols, out_cols), bf),
            pltpu.VMEM((rows, chunk), bf),
            pltpu.VMEM((2 * rows, width), bf),
            pltpu.VMEM((1, width), f32),
            pltpu.VMEM(table.shape, f32),
            pltpu.VMEM((heads // 2, q_rows, span), f32),
            pltpu.VMEM((pairs, 2 * rows, lanes), bf),
            pltpu.VMEM((pairs, 3 * rows, 2 * lanes), bf),
            pltpu.VMEM((1, 3 * rows), jnp.int32),
            pltpu.VMEM((2 * rows // q_rows, q_rows, span), f32),
            pltpu.VMEM((rows // q_rows, 2, q_rows, cols // 2), bf),
            pltpu.VMEM((rows // q_rows, q_rows, cols // 2), bf),
            pltpu.VMEM((n_tp, rows, cols), bf),
            dma((2, pairs, 3)),
            dma((pairs, 3)),
            dma((n_tp,)),
            dma((2 * n_tp,)),
            dma(()),
            dma((4,)),
            dma((n_tp - 1,)),
            dma((n_tp - 1,)),
            dma(()),
            dma((3,)),
            dma((3,)),
            dma(()),
            dma((4, 3)),
            dma((4,)),
            dma((4, 2, n_sp)),
            dma((4, n_sp)),
            dma((2, 3, 2 * n_tp + 1)),
            dma((2, 2, 2 * n_tp + 1)),
            dma((pairs + 1,)),
            dma((pairs + 1,)),
            dma((3, rows // q_rows, 2)),
            dma((3, rows // q_rows, 2)),
        ],
        compiler_params=pltpu.CompilerParams(
            collective_id=0, has_side_effects=True, vmem_limit_bytes=60 * 1024 * 1024
        ),
    )(documents[None, :], norm_gain, table, tokens, w_key[0], w_value[0], w_query[0], w_out[0])


def fits_one(mesh):
    return mesh.shape["tp"] == 4 and mesh.shape["sp"] == 2 * mesh.shape["tp"]


def solution(mesh):
    n_sp, n_tp = mesh.shape["sp"], mesh.shape["tp"]
    run = functools.partial(body_one, n_sp, n_tp) if fits_one(mesh) else body
    in_specs = (
        P("sp", None),
        P("sp"),
        P(),
        P(None, "sp", "tp"),
        P(None, "sp", "tp"),
        P(None, "sp", "tp"),
        P(None, None, "sp"),
        P(None, "tp", None),
    )
    out_specs = P("sp", None)
    return jax.shard_map(run, mesh=mesh, in_specs=in_specs, out_specs=out_specs, check_vma=False)
```

```python
import functools

import jax
import jax.numpy as jnp
from jax import lax
from jax.experimental import pallas as pl
from jax.experimental.pallas import tpu as pltpu
from jax.sharding import PartitionSpec as P

HEAD_DIM = 64
SEG = 64
LEFT = 4
REL_CLIP = 128


EPS = 1e-06


def passed_along(x, axis, by):
    length = lax.axis_size(axis)
    pairs = [(i, i + by) for i in range(length) if 0 <= i + by < length]
    return lax.ppermute(x, axis, pairs)


def banded_bias(bias_table, query_rows, key_rows, reach_rows):
    span_len = query_rows + key_rows - 1
    steps_back = jnp.arange(span_len, dtype=jnp.int32) - (key_rows - 1) + reach_rows
    lookup = jnp.clip(steps_back, -REL_CLIP, REL_CLIP) + REL_CLIP
    bias_line = jnp.take(bias_table, lookup, axis=1)
    reversed_line = bias_line[:, ::-1]
    repeated = jnp.tile(reversed_line, (1, query_rows))
    skewed = repeated[:, query_rows - 1 : query_rows - 1 + query_rows * (span_len - 1)]
    skewed = skewed.reshape(bias_table.shape[0], query_rows, span_len - 1)
    return skewed[:, :, :key_rows]


def attend(queries, keys_all, values_all, query_pos, key_pos, query_doc, key_doc, bias_table):
    query_rows = queries.shape[0]
    key_rows = keys_all.shape[0]
    reach_rows = key_rows - query_rows
    scores = jnp.einsum(
        "qhe,khe->hqk", queries, keys_all, preferred_element_type=jnp.float32
    ) * HEAD_DIM ** (-0.5)
    scores = scores + banded_bias(bias_table, query_rows, key_rows, reach_rows)
    query_seg = query_pos // SEG
    key_seg = key_pos // SEG
    allowed = (
        (key_pos[None, :] >= 0)
        & (key_seg[None, :] <= query_seg[:, None])
        & (key_seg[None, :] >= query_seg[:, None] - LEFT)
        & (key_doc[None, :] == query_doc[:, None])
    )
    scores = jnp.where(allowed[None], scores, -1e30)
    peak = jnp.max(scores, axis=-1, keepdims=True)
    raised = jnp.exp(scores - peak)
    weights_bf = (raised / jnp.sum(raised, axis=-1, keepdims=True)).astype(jnp.bfloat16)
    return jnp.einsum(
        "hqk,khe->qhe", weights_bf, values_all, preferred_element_type=jnp.float32
    ).astype(jnp.bfloat16)


def body(tokens, documents, norm_gain, w_query, w_key, w_value, w_out, rel_bias):
    local_rows = tokens.shape[0]
    reach_rows = LEFT * SEG
    width_local = w_query.shape[2]
    heads_local = width_local // HEAD_DIM
    offset = lax.axis_index("sp") * local_rows
    query_pos = offset + jnp.arange(local_rows, dtype=jnp.int32)
    key_pos = offset - reach_rows + jnp.arange(reach_rows + local_rows, dtype=jnp.int32)
    widened = tokens.astype(jnp.float32)
    normed = (
        widened
        * lax.rsqrt(jnp.mean(widened * widened, axis=-1, keepdims=True) + EPS)
        * norm_gain[0]
    ).astype(jnp.bfloat16)
    query_sum = jnp.dot(
        normed,
        lax.all_gather(w_query[0], "sp", axis=0, tiled=True),
        preferred_element_type=jnp.float32,
    )
    key_sum = jnp.dot(
        normed,
        lax.all_gather(w_key[0], "sp", axis=0, tiled=True),
        preferred_element_type=jnp.float32,
    )
    value_sum = jnp.dot(
        normed,
        lax.all_gather(w_value[0], "sp", axis=0, tiled=True),
        preferred_element_type=jnp.float32,
    )
    queries = query_sum.astype(jnp.bfloat16)
    keys_own = key_sum.astype(jnp.bfloat16)
    values_own = value_sum.astype(jnp.bfloat16)
    prior_keys, prior_values, prior_docs = passed_along((keys_own, values_own, documents), "sp", 1)
    keys_all = jnp.concatenate([prior_keys, keys_own], axis=0)
    values_all = jnp.concatenate([prior_values, values_own], axis=0)
    key_doc = jnp.concatenate([prior_docs, documents], axis=0)
    attended = attend(
        queries.reshape(local_rows, heads_local, HEAD_DIM),
        keys_all.reshape(reach_rows + local_rows, heads_local, HEAD_DIM),
        values_all.reshape(reach_rows + local_rows, heads_local, HEAD_DIM),
        query_pos,
        key_pos,
        documents,
        key_doc,
        rel_bias[0],
    ).reshape(local_rows, width_local)
    all_heads = lax.all_gather(attended, "tp", axis=1, tiled=True)
    return (
        widened
        + jnp.dot(
            all_heads,
            lax.all_gather(w_out[0], "sp", axis=1, tiled=True),
            preferred_element_type=jnp.float32,
        )
    ).astype(jnp.bfloat16)


MESH = pl.DeviceIdType.MESH
TOK, OUT = range(2)
UP, DOWN, ACROSS = range(3)
W0, W1, A0, A1 = range(4)
NEG = -1e30


def plane_of(t):
    c = t % 2
    return 3 * c + (t // 2) * (1 - 2 * c)


def part_for(z):
    return 2 * (((z + 1) // 2) % 2) + z // 2


def layer_kernel(
    n_sp, n_tp, doc_in, gain_in, table_in, x_in, wk_in, wv_in, wq_in, wo_in, out_ref,
    w_own, w_relay, w_all, wo_all, tok, aid, wo_aid, resid, normed, gain, table, bias, q_buf, kv_all, docs_all, mask,
    att_own, att_relay, att_all,
    own_sem, loc_sem, out_sem, tok_sem, aid_sem, aid_send, wo_aid_sem, wo_aid_send, res_sem, small_sem, line_send, line_recv, hop_send, relay_recv, rep_send, rep_recv,
    cast_send, cast_recv, across_recv, halo_send, halo_recv, tp_send, tp_recv,
):
    rows, width = tok.shape[1:]
    depth, cols = wk_in.shape
    half_cols = cols // 2
    lanes = 2 * HEAD_DIM
    pairs = half_cols // lanes
    q_rows, span = 2 * SEG, (LEFT + 2) * SEG
    chunk = width // n_tp
    nz = n_sp // 2
    pieces = 2 * n_tp
    aids = n_tp
    piece = rows // pieces
    s = lax.axis_index("sp")
    t = lax.axis_index("tp")
    z, x = s // 2, s % 2
    mate = s + 1 - 2 * x
    ty, tc = t // 2, t % 2
    t_core = t + 1 - 2 * tc
    t_y = (1 - ty) * 2 + tc
    t_far = (1 - ty) * 2 + 1 - tc
    home, home_y = plane_of(t), plane_of(t_y)
    first_entry, second_entry = z == home, z == home_y
    entry = first_entry | second_entry
    gap = z - home
    is_first = 1 - (gap * gap + n_sp) // (n_sp + 1)
    x_mine = x * is_first + (1 - x) * (1 - is_first)
    own_in = (wk_in, wv_in, wq_in)
    has_up, has_down = z < nz - 1, z > 0

    def at_multiple(start, size, step):
        return pl.ds(pl.multiple_of(start, step), size)

    def weight_cols(which, p):
        return at_multiple(which * half_cols + p * lanes, lanes, lanes)

    def kind_cols(kind):
        return pl.ds(kind * lanes, lanes)

    def own_copy(i, p, kind):
        which = x if i == 0 else 1 - x
        return pltpu.make_async_copy(
            own_in[kind].at[:, weight_cols(which, p)], w_own.at[i, p, :, kind_cols(kind)], own_sem.at[i, p]
        )

    def local_copy(p, kind):
        return pltpu.make_async_copy(
            own_in[kind].at[:, weight_cols(x, p)],
            w_all.at[p, at_multiple(s * depth, depth, depth), kind_cols(kind)], loc_sem.at[p],
        )

    tok_copy = pltpu.make_async_copy(x_in, tok.at[x], tok_sem)

    def out_copy(r):
        return pltpu.make_async_copy(wo_in.at[pl.ds(r * cols, cols), :], wo_all.at[2 * r + x], out_sem.at[r])

    doc_copy = pltpu.make_async_copy(doc_in, docs_all.at[:, at_multiple((1 + x) * rows, rows, rows)], small_sem.at[0])
    gain_copy = pltpu.make_async_copy(gain_in, gain, small_sem.at[1])
    table_copy = pltpu.make_async_copy(table_in, table, small_sem.at[2])
    resid_copy = pltpu.make_async_copy(x_in.at[:, at_multiple(home_y * chunk, chunk, chunk)], resid, res_sem)

    gain_copy.start()

    @pl.when(first_entry)
    def _():
        doc_copy.start()
        tok_copy.start()
        table_copy.start()

    for p in range(pairs):
        for i in (1, 0):
            for kind in range(3):
                own_copy(i, p, kind).start()

    @pl.when(first_entry)
    def _():
        for p in range(pairs):
            for kind in range(3):
                local_copy(p, kind).start()

    outer = (z == 0) | (z == nz - 1)
    inner = jnp.logical_not(outer)
    lower = z < nz // 2
    aid_copy = pltpu.make_async_copy(x_in.at[pl.ds(rows - 4 * piece, 4 * piece), :], aid, aid_sem)

    def wo_aid_copy(r):
        return pltpu.make_async_copy(wo_in.at[pl.ds(r * cols, cols), :], wo_aid.at[r - 1], wo_aid_sem.at[r - 1])

    aide = inner & (z == plane_of(t_far))

    @pl.when(aide)
    def _():
        for r in range(1, n_tp):
            wo_aid_copy(r).start()

    @pl.when(second_entry)
    def _():
        pl.when(inner)(lambda: aid_copy.start())

        for r in range(n_tp):
            out_copy(r).start()

    resid_copy.start()

    def remote(src, dst, send, recv, **where):
        return pltpu.make_async_remote_copy(
            src_ref=src, dst_ref=dst, send_sem=send, recv_sem=recv, device_id=where, device_id_type=MESH
        )

    def slot(ch, block):
        if ch < A0:
            return w_all.at[ch - W0, at_multiple(block * depth, depth, depth), :]
        return att_all.at[
            part_for(block // 2), pl.ds((ch - A0) * q_rows, q_rows), at_multiple((block % 2) * half_cols, half_cols, half_cols)
        ]

    def own_ref(ch, i):
        return w_own.at[i, ch - W0] if ch < A0 else att_own.at[ch - A0, x if i == 0 else 1 - x]

    def relay_ref(ch):
        return w_relay.at[ch - W0] if ch < A0 else att_relay.at[ch - A0]

    def direct(ch):
        return remote(own_ref(ch, 0), slot(ch, s), hop_send.at[ch, 0], rep_recv.at[ch, s], sp=2 * home + x)

    def cross_in(ch):
        return remote(own_ref(ch, 1), slot(ch, s), hop_send.at[ch, 1], rep_recv.at[ch, s], sp=mate, tp=t_y)

    def cross_relay(ch):
        return remote(own_ref(ch, 1), relay_ref(ch), hop_send.at[ch, 1], relay_recv.at[ch], sp=mate, tp=t_y)

    def relay(ch):
        return remote(relay_ref(ch), slot(ch, mate), hop_send.at[ch, 2], rep_recv.at[ch, mate], sp=2 * home_y + x)

    def to_y(ch, block):
        return remote(slot(ch, block), slot(ch, block), rep_send.at[ch, 0], rep_recv.at[ch, block], tp=t_y)

    def to_core(ch, block):
        return remote(slot(ch, block), slot(ch, block), rep_send.at[ch, 1], rep_recv.at[ch, block], tp=t_core)

    def send_cross(ch):
        pl.when(first_entry)(lambda: cross_in(ch).start())
        pl.when(jnp.logical_not(first_entry))(lambda: cross_relay(ch).start())

    def send_direct(ch):
        pl.when(jnp.logical_not(first_entry))(lambda: direct(ch).start())

    def send_relay(ch):
        @pl.when(jnp.logical_not(second_entry))
        def _():
            cross_relay(ch).wait_recv()
            relay(ch).start()

    planes = [0]
    for d in range(1, nz):
        planes += [-d, d]

    def valid(off):
        return (z + off >= 0) & (z + off < nz)

    def mine(ch, off):
        @pl.when(entry & valid(off))
        def _():
            block = 2 * (z + off) + x_mine
            if off == 0:
                pl.when(jnp.logical_not(first_entry))(lambda: to_y(ch, block).wait_recv())
                if ch < A0:
                    @pl.when(first_entry)
                    def _():
                        wide = wk_in.at[:, pl.ds(0, 3 * lanes)]
                        pltpu.make_async_copy(wide, slot(ch, s), loc_sem.at[ch - W0]).wait()
            else:
                to_y(ch, block).wait_recv()
            to_y(ch, block).start()
            to_core(ch, block).start()

    def theirs(ch, off):
        @pl.when(valid(off))
        def _():
            @pl.when(entry)
            def _():
                block = 2 * (z + off) + 1 - x_mine
                to_y(ch, block).wait_recv()
                to_core(ch, block).start()

            @pl.when(jnp.logical_not(entry))
            def _():
                for i in range(2):
                    to_core(ch, 2 * (z + off) + i).wait_recv()

    def spread(ch, first, last):
        for i in range(first, last + 1):
            if i < len(planes):
                mine(ch, planes[i])
            if i > 0:
                theirs(ch, planes[i - 1])

    def drain(ch):
        pl.when(jnp.logical_not(first_entry))(lambda: direct(ch).wait_send())
        cross_relay(ch).wait_send()
        pl.when(jnp.logical_not(second_entry))(lambda: relay(ch).wait_send())

        @pl.when(entry)
        def _():
            if ch < A0:
                some, every = w_all.at[ch - W0, pl.ds(0, nz * depth), :], w_all.at[ch - W0]
            else:
                some, every = att_all.at[0], att_all.at[pl.ds(0, 2)]
            remote(some, some, rep_send.at[ch, 0], rep_recv.at[ch, 0], tp=t_y).wait_send()
            remote(every, every, rep_send.at[ch, 1], rep_recv.at[ch, 0], tp=t_core).wait_send()

    def cast_ref(kind, which, r):
        if kind == OUT:
            return wo_all.at[2 * r + which]
        if r == pieces:
            return docs_all.at[:, at_multiple((1 + which) * rows, rows, rows)]
        return tok.at[which, pl.ds(r * piece, piece), :]

    def group_of(kind, r):
        if kind == OUT:
            return 3 if r == 0 else 4
        return 2 if r == pieces else int(r >= pieces - aids)

    def line_in(kind, r):
        return cast_recv.at[r if kind == TOK else pieces + 1 + r]

    def move(kind, way, r):
        ref = cast_ref(kind, x, r)
        arrive = across_recv.at[(0, 0, 1, 2, 2)[group_of(kind, r)]] if way == ACROSS else line_in(kind, r)
        return remote(ref, ref, cast_send.at[group_of(kind, r), way], arrive, sp=(s + 2, s - 2, mate)[way])

    aid_rows = aids * piece
    whole = (
        tok.at[0, pl.ds(0, rows - aid_rows), :], tok.at[0, pl.ds(0, aid_rows), :], docs_all.at[:, pl.ds(0, rows)],
        wo_all.at[0], wo_all.at[pl.ds(0, n_tp - 1)],
    )

    def across_all(i):
        ref = (tok.at[1 - x], docs_all.at[:, at_multiple((2 - x) * rows, rows, rows)], wo_all.at[pl.ds(0, n_tp)])[i]
        return remote(ref, ref, cast_send.at[0, ACROSS], across_recv.at[i], sp=mate)

    centers = (home, home_y)

    def aided(kind, r):
        return pieces - aids <= r < pieces if kind == TOK else r > 0

    def goes(kind, way, r):
        ok = (z >= centers[kind]) & has_up if way == UP else (z <= centers[kind]) & has_down
        if aided(kind, r):
            near = jnp.logical_not(lower) if way == UP else lower
            ok = ok & jnp.logical_not((z == centers[kind]) & inner & near)
        return ok

    def aid_move(i):
        r = pieces - aids + i
        return remote(
            aid.at[pl.ds(i * piece, piece), :], cast_ref(TOK, x, r), aid_send, line_in(TOK, r),
            sp=s + 2 - 4 * (1 - z // (nz // 2)), tp=t_y,
        )

    def wo_aid_move(r):
        return remote(
            wo_aid.at[r - 1], cast_ref(OUT, x, r), wo_aid_send.at[r - 1], line_in(OUT, r),
            sp=s + 2 - 4 * (1 - z // (nz // 2)), tp=t_core,
        )

    def cast_along(kind, r):
        for way in (UP, DOWN):
            pl.when(goes(kind, way, r))(lambda: move(kind, way, r).start())

    def cast_send_on(kind, r):
        cast_along(kind, r)
        move(kind, ACROSS, r).start()

    def cast_source(kind, r):
        if r == pieces and kind == TOK:
            doc_copy.wait()
            cast_send_on(kind, r)
            return
        if kind == OUT:
            out_copy(r).wait()
        elif r == 0:
            tok_copy.wait()
        cast_send_on(kind, r)

    def cast_forward(kind, r):
        @pl.when(z != centers[kind])
        def _():
            move(kind, UP, r).wait_recv()
            cast_send_on(kind, r)

    def cast_drain():
        for g, (kind, r) in enumerate(((TOK, 0), (TOK, pieces - 1), (TOK, pieces), (OUT, 0), (OUT, 1))):
            def done(way):
                remote(whole[g], whole[g], cast_send.at[g, way], line_in(kind, r), sp=mate).wait_send()

            for way in (UP, DOWN):
                pl.when(goes(kind, way, r))(lambda: done(way))
            done(ACROSS)

    line_targets = (t_core, t_y, t_far)

    def line_copy(i):
        return remote(table, table, line_send.at[i], line_recv, tp=line_targets[i])

    has_next, has_prev = home < nz - 1, home > 0

    def halo(i):
        if i == pairs:
            src, dst = docs_all.at[:, pl.ds(2 * rows, rows)], docs_all.at[:, pl.ds(0, rows)]
        else:
            src, dst = kv_all.at[i, pl.ds(2 * rows, rows), :], kv_all.at[i, pl.ds(0, rows), :]
        return remote(src, dst, halo_send.at[i], halo_recv.at[i], tp=part_for((home + 1) % nz))

    barrier = pltpu.get_barrier_semaphore()
    for d in range(1, nz):
        pl.semaphore_signal(
            barrier, inc=1, device_id={"sp": lax.rem(s + 2 * d, n_sp)}, device_id_type=MESH
        )
    for peer in (t_core, t_y, t_far):
        pl.semaphore_signal(barrier, inc=1, device_id={"tp": peer}, device_id_type=MESH)
    for peer in (t, t_y):
        pl.semaphore_signal(barrier, inc=1, device_id={"sp": mate, "tp": peer}, device_id_type=MESH)
    pl.semaphore_signal(
        barrier, inc=1, device_id={"sp": s + 2 - 4 * (z % 2), "tp": t_y}, device_id_type=MESH
    )
    pl.semaphore_signal(
        barrier, inc=1, device_id={"sp": s + 2 - 4 * (z % 2), "tp": t_core}, device_id_type=MESH
    )
    pl.semaphore_wait(barrier, nz + 6)

    for p in range(pairs):
        for i in (1, 0):
            wide = wk_in.at[:, pl.ds(0, 3 * lanes)]
            pltpu.make_async_copy(wide, w_own.at[i, p], own_sem.at[i, p]).wait()
            (send_direct, send_cross)[i](W0 + p)

    @pl.when(first_entry)
    def _():
        for r in (pieces,) + tuple(range(pieces)):
            cast_source(TOK, r)
        table_copy.wait()
        for i in range(3):
            line_copy(i).start()

    def out_along(r):
        out_copy(r).wait()
        cast_along(OUT, r)

    def out_near(r):
        pl.when(goes(OUT, UP, r) & jnp.logical_not(lower))(lambda: move(OUT, UP, r).start())
        pl.when(goes(OUT, DOWN, r) & lower)(lambda: move(OUT, DOWN, r).start())

    def out_far(r):
        pl.when(goes(OUT, UP, r) & lower)(lambda: move(OUT, UP, r).start())
        pl.when(goes(OUT, DOWN, r) & jnp.logical_not(lower))(lambda: move(OUT, DOWN, r).start())

    def out_across(r):
        move(OUT, ACROSS, r).start()

    def out_pass(r):
        @pl.when(z != home_y)
        def _():
            move(OUT, UP, r).wait_recv()
            cast_along(OUT, r)

    @pl.when(second_entry)
    def _():
        @pl.when(inner)
        def _():
            aid_copy.wait()
            for i in range(aids):
                aid_move(i).start()

        @pl.when(outer)
        def _():
            for r in range(n_tp):
                out_along(r)

    @pl.when(has_prev == False)
    def _():
        docs_all[:, pl.ds(0, rows)] = jnp.full((1, rows), -1, jnp.int32)
        for p in range(pairs):
            kv_all[p, pl.ds(0, rows), :] = jnp.zeros((rows, 2 * lanes), jnp.bfloat16)

    def around(d):
        return (0,) if d == 0 else (-d, d)

    def pass_mine(ch, d):
        for off in around(d):
            mine(ch, off)

    def pass_theirs(ch, d):
        for off in around(d):
            theirs(ch, off)

    @pl.when(first_entry)
    def _():
        pass_mine(W0, 0)
        pass_mine(W1, 0)
        send_relay(W0)
        send_relay(W1)
        for ch in (W0, W1):
            for d in range(1, nz):
                pass_mine(ch, d)

        @pl.when(inner)
        def _():
            for r in range(n_tp):
                out_pass(r)
                if r < 2:
                    out_across(r)

        @pl.when(outer)
        def _():
            out_pass(0)
            out_across(0)

        for ch in (W0, W1):
            for d in range(nz):
                pass_theirs(ch, d)

    @pl.when(second_entry)
    def _():
        pass_mine(W0, 0)
        cast_forward(TOK, pieces)
        for r in range(0, 2):
            cast_forward(TOK, r)

        @pl.when(inner)
        def _():
            out_copy(0).wait()
            out_near(0)

        out_across(0)
        pass_mine(W1, 0)
        for r in range(2, 4):
            cast_forward(TOK, r)
        pl.when(inner)(lambda: out_copy(1).wait())
        out_across(1)
        pass_mine(W0, 1)
        pass_mine(W1, 1)
        for r in range(4, 6):
            cast_forward(TOK, r)
        pass_mine(W0, 2)
        pass_mine(W1, 2)
        for r in range(6, 8):
            cast_forward(TOK, r)
        pass_mine(W0, 3)
        pass_mine(W1, 3)

        @pl.when(inner)
        def _():
            for r in range(n_tp):
                if r >= 2:
                    out_copy(r).wait()
                out_far(r)

        for ch in (W0, W1):
            for d in range(nz):
                pass_theirs(ch, d)

    @pl.when(jnp.logical_not(entry))
    def _():
        send_relay(W0)
        send_relay(W1)
        for r in (pieces,) + tuple(range(pieces)):
            cast_forward(TOK, r)

        @pl.when(aide)
        def _():
            for r in range(1, n_tp):
                wo_aid_copy(r).wait()
                wo_aid_move(r).start()

        pl.when(inner)(lambda: out_pass(0))
        for ch in (W0, W1):
            for d in range(nz):
                pass_theirs(ch, d)


    gain_copy.wait()

    def normalize(which):
        wide = tok[which].astype(jnp.float32)
        normed[at_multiple(which * rows, rows, rows), :] = (
            wide * lax.rsqrt(jnp.mean(wide * wide, axis=-1, keepdims=True) + EPS) * gain[...]
        ).astype(jnp.bfloat16)

    normalize(x)

    heads = half_cols // HEAD_DIM
    blocks = 2 * rows // q_rows

    pl.when(jnp.logical_not(first_entry))(lambda: line_copy(0).wait_recv())
    q_seg = lax.broadcasted_iota(jnp.int32, (q_rows, span), 0) // SEG
    k_seg = lax.broadcasted_iota(jnp.int32, (q_rows, span), 1) // SEG
    near = (k_seg >= q_seg) & (k_seg <= q_seg + LEFT)
    length = table.shape[1]
    line_len = (LEFT + 4) * SEG
    entry_of = lax.broadcasted_iota(jnp.int32, (length, line_len), 0)
    back = LEFT * SEG - lax.broadcasted_iota(jnp.int32, (length, line_len), 1)
    back = jnp.where(back < -REL_CLIP, REL_CLIP, jnp.minimum(back, REL_CLIP))
    pick = (entry_of == back + REL_CLIP).astype(jnp.float32)
    lines = jnp.dot(table[...], pick, precision=lax.Precision.HIGHEST, preferred_element_type=jnp.float32)
    lines = jnp.where(x == 0, lines[:heads], lines[heads:])
    for h in range(heads):
        line = jnp.broadcast_to(lines[h : h + 1, :], (q_rows, line_len))
        skew = pltpu.roll(line, 0, 1, stride=1, stride_axis=0)
        bias[h] = jnp.where(near, skew[:, :span], NEG)

    def project(which):
        own = at_multiple(which * rows, rows, rows)
        for p in range(pairs):
            made = jnp.dot(normed[own, :], w_all[p], preferred_element_type=jnp.float32).astype(jnp.bfloat16)
            kv_all[p, at_multiple((1 + which) * rows, rows, rows), :] = made[:, : 2 * lanes]
            q_buf[p, own, :] = (made[:, 2 * lanes :].astype(jnp.float32) * HEAD_DIM ** (-0.5)).astype(jnp.bfloat16)

    def send_halo():
        for p in range(pairs):
            halo(p).start()

    project(x)
    pl.when(has_next & (x == 1))(send_halo)
    middle = jnp.logical_not(entry) & inner

    pl.when(middle)(lambda: out_pass(1))
    for i in range(2):
        across_all(i).wait_recv()
    pl.when(has_next)(lambda: halo(pairs).start())
    normalize(1 - x)
    late = jnp.logical_not(second_entry) & outer
    project(1 - x)
    pl.when(has_next & (x == 0))(send_halo)

    low = lax.broadcasted_iota(jnp.int32, (q_rows, lanes), 1) < HEAD_DIM
    eye = lax.broadcasted_iota(jnp.int32, (q_rows, q_rows), 0) == lax.broadcasted_iota(jnp.int32, (q_rows, q_rows), 1)

    def make_mask(j):
        q_docs = docs_all[pl.ds(0, 1), pl.ds(rows + j * q_rows, q_rows)].astype(jnp.float32)
        k_docs = docs_all[pl.ds(0, 1), pl.ds(j * q_rows, span)].astype(jnp.float32)
        column = jnp.sum(jnp.where(eye, jnp.broadcast_to(q_docs, (q_rows, q_rows)), 0.0), axis=1, keepdims=True)
        mask[j] = jnp.where(column == k_docs, 0.0, NEG)

    def attend_rows(g):
        keys, queries = pl.ds(g * q_rows, span), pl.ds(g * q_rows, q_rows)
        found = []
        for p in range(pairs):
            q_pair = q_buf[p, queries, :]
            k_pair = kv_all[p, keys, pl.ds(0, lanes)]
            v_pair = kv_all[p, keys, pl.ds(lanes, lanes)]
            both = []
            for half in range(2):
                on = low if half == 0 else jnp.logical_not(low)
                q_one = jnp.where(on, q_pair, jnp.zeros_like(q_pair))
                score = lax.dot_general(q_one, k_pair, (((1,), (1,)), ((), ())), preferred_element_type=jnp.float32)
                score = score + bias[2 * p + half] + mask[g]
                raised = jnp.exp(score - jnp.max(score, axis=-1, keepdims=True))
                total = jnp.sum(raised, axis=-1, keepdims=True)
                both.append(jnp.dot(raised.astype(jnp.bfloat16), v_pair, preferred_element_type=jnp.float32) / total)
            found.append(jnp.where(low, both[0], both[1]).astype(jnp.bfloat16))
        return jnp.concatenate(found, axis=1)

    per = blocks // 2

    def attend_step(j, which):
        found = attend_rows(which * per + j)
        att_own[j, which] = found

        @pl.when(first_entry & (x == which))
        def _():
            att_all[t, pl.ds(j * q_rows, q_rows), at_multiple(x * half_cols, half_cols, half_cols)] = found

        pl.when(x == which)(lambda: send_direct(A0 + j))
        pl.when(x != which)(lambda: send_cross(A0 + j))

    for g in range(per, blocks):
        make_mask(g)
    attend_step(0, 1)
    pl.when(middle)(lambda: out_pass(2))
    attend_step(1, 1)
    pl.when(middle)(lambda: out_pass(3))

    @pl.when(has_prev)
    def _():
        for i in (pairs,) + tuple(range(pairs)):
            halo(i).wait_recv()

    for g in range(per):
        make_mask(g)
    attend_step(0, 0)
    attend_step(1, 0)
    third = jnp.logical_not(entry)
    pl.when(third & outer)(lambda: out_pass(0))
    pl.when(third)(lambda: out_across(0))
    pl.when(first_entry & outer)(lambda: out_pass(1))
    pl.when(first_entry & outer)(lambda: out_across(1))
    send_relay(A0)
    send_relay(A1)
    pl.when(third & outer)(lambda: out_pass(1))
    pl.when(third)(lambda: out_across(1))
    swift = jnp.logical_not(late)

    @pl.when(swift)
    def _():
        out_across(2)
        out_across(3)

    for d in range(nz):
        for ch in (A0, A1):
            pass_mine(ch, d)

    @pl.when(late)
    def _():
        for r in (2, 3):
            out_pass(r)
            out_across(r)

    half_chunk = chunk // 2

    def result(which, j, i):
        cut = at_multiple(which * chunk + i * half_chunk, half_chunk, half_chunk)
        return out_ref.at[pl.ds(j * q_rows, q_rows), cut]

    def tp_move(way, j, i):
        which, target = ((home_y, t_y), (home_y, t_core), (home, t_core))[way]
        ref = result(which, j, i)
        return remote(ref, ref, tp_send.at[way], tp_recv.at[way, j, i], tp=target)

    def out_project(j, i):
        part = pl.ds(j * q_rows, q_rows)
        made = jnp.zeros((q_rows, half_chunk), jnp.float32)
        for r in range(n_tp):
            made = made + jnp.dot(att_all[r, part, :], wo_all[2 * r + i], preferred_element_type=jnp.float32)
        rest = resid[part, at_multiple(i * half_chunk, half_chunk, half_chunk)].astype(jnp.float32)
        result(home_y, j, i)[...] = (rest + made).astype(jnp.bfloat16)
        tp_move(0, j, i).start()
        tp_move(1, j, i).start()

    resid_copy.wait()
    for j in range(per):
        for d in range(nz):
            pass_theirs(A0 + j, d)
        out_project(j, x)
    across_all(2).wait_recv()
    for j in range(per):
        out_project(j, 1 - x)
    quarters = [(j, i) for i in (x, 1 - x) for j in range(per)]
    for q in quarters:
        tp_move(0, *q).wait_recv()
        tp_move(2, *q).start()
    for q in quarters:
        tp_move(1, *q).wait_recv()
        tp_move(2, *q).wait_recv()

    for ch in range(4):
        drain(ch)
    cast_drain()

    @pl.when(second_entry & inner)
    def _():
        remote(aid, whole[1], aid_send, line_in(TOK, 0), tp=t_y).wait_send()

    @pl.when(aide)
    def _():
        for r in range(1, n_tp):
            wo_aid_move(r).wait_send()


    @pl.when(first_entry)
    def _():
        for i in range(3):
            line_copy(i).wait_send()

    @pl.when(has_next)
    def _():
        for i in range(pairs + 1):
            halo(i).wait_send()
    for way in range(3):
        ref = out_ref.at[:, pl.ds(0, chunk)]
        remote(ref, ref, tp_send.at[way], tp_recv.at[way, 0, 0], tp=t_y).wait_send()


def body_one(n_sp, n_tp, tokens, documents, norm_gain, w_query, w_key, w_value, w_out, rel_bias):
    rows, width = tokens.shape
    depth, cols = w_query.shape[1:]
    heads = cols // HEAD_DIM
    out_cols = w_out.shape[2]
    chunk = width // n_tp
    lanes = 2 * HEAD_DIM
    pairs = cols // 2 // lanes
    table = rel_bias[0]
    bf, f32 = jnp.bfloat16, jnp.float32
    hbm = pl.BlockSpec(memory_space=pl.ANY)
    dma = pltpu.SemaphoreType.DMA
    q_rows, span = 2 * SEG, (LEFT + 2) * SEG
    return pl.pallas_call(
        functools.partial(layer_kernel, n_sp, n_tp),
        out_shape=pltpu.VMEM((rows, width), bf),
        in_specs=[hbm] * 8,
        out_specs=pl.BlockSpec(memory_space=pltpu.VMEM),
        scratch_shapes=[
            pltpu.VMEM((2, pairs, depth, 3 * lanes), bf),
            pltpu.VMEM((pairs, depth, 3 * lanes), bf),
            pltpu.VMEM((pairs, n_sp * depth, 3 * lanes), bf),
            pltpu.VMEM((n_sp, cols, out_cols), bf),
            pltpu.VMEM((2, rows, width), bf),
            pltpu.VMEM((4 * rows // (2 * n_tp), width), bf),
            pltpu.VMEM((n_tp - 1, cols, out_cols), bf),
            pltpu.VMEM((rows, chunk), bf),
            pltpu.VMEM((2 * rows, width), bf),
            pltpu.VMEM((1, width), f32),
            pltpu.VMEM(table.shape, f32),
            pltpu.VMEM((heads // 2, q_rows, span), f32),
            pltpu.VMEM((pairs, 2 * rows, lanes), bf),
            pltpu.VMEM((pairs, 3 * rows, 2 * lanes), bf),
            pltpu.VMEM((1, 3 * rows), jnp.int32),
            pltpu.VMEM((2 * rows // q_rows, q_rows, span), f32),
            pltpu.VMEM((rows // q_rows, 2, q_rows, cols // 2), bf),
            pltpu.VMEM((rows // q_rows, q_rows, cols // 2), bf),
            pltpu.VMEM((n_tp, rows, cols), bf),
            dma((2, pairs)),
            dma((pairs,)),
            dma((n_tp,)),
            dma(()),
            dma(()),
            dma(()),
            dma((n_tp - 1,)),
            dma((n_tp - 1,)),
            dma(()),
            dma((3,)),
            dma((3,)),
            dma(()),
            dma((4, 3)),
            dma((4,)),
            dma((4, 2)),
            dma((4, n_sp)),
            dma((5, 3)),
            dma((3 * n_tp + 1,)),
            dma((3,)),
            dma((pairs + 1,)),
            dma((pairs + 1,)),
            dma((3,)),
            dma((3, rows // q_rows, 2)),
        ],
        compiler_params=pltpu.CompilerParams(
            collective_id=0, has_side_effects=True, vmem_limit_bytes=60 * 1024 * 1024
        ),
    )(documents[None, :], norm_gain, table, tokens, w_key[0], w_value[0], w_query[0], w_out[0])


def fits_one(mesh):
    return mesh.shape["tp"] == 4 and mesh.shape["sp"] == 2 * mesh.shape["tp"]


def solution(mesh):
    n_sp, n_tp = mesh.shape["sp"], mesh.shape["tp"]
    run = functools.partial(body_one, n_sp, n_tp) if fits_one(mesh) else body
    in_specs = (
        P("sp", None),
        P("sp"),
        P(),
        P(None, "sp", "tp"),
        P(None, "sp", "tp"),
        P(None, "sp", "tp"),
        P(None, None, "sp"),
        P(None, "tp", None),
    )
    out_specs = P("sp", None)
    return jax.shard_map(run, mesh=mesh, in_specs=in_specs, out_specs=out_specs, check_vma=False)
```

```python
import functools

import jax
import jax.numpy as jnp
from jax import lax
from jax.experimental import pallas as pl
from jax.experimental.pallas import tpu as pltpu
from jax.sharding import PartitionSpec as P

HEAD_DIM = 64
SEG = 64
LEFT = 4
REL_CLIP = 128


EPS = 1e-06


def passed_along(x, axis, by):
    length = lax.axis_size(axis)
    pairs = [(i, i + by) for i in range(length) if 0 <= i + by < length]
    return lax.ppermute(x, axis, pairs)


def banded_bias(bias_table, query_rows, key_rows, reach_rows):
    span_len = query_rows + key_rows - 1
    steps_back = jnp.arange(span_len, dtype=jnp.int32) - (key_rows - 1) + reach_rows
    lookup = jnp.clip(steps_back, -REL_CLIP, REL_CLIP) + REL_CLIP
    bias_line = jnp.take(bias_table, lookup, axis=1)
    reversed_line = bias_line[:, ::-1]
    repeated = jnp.tile(reversed_line, (1, query_rows))
    skewed = repeated[:, query_rows - 1 : query_rows - 1 + query_rows * (span_len - 1)]
    skewed = skewed.reshape(bias_table.shape[0], query_rows, span_len - 1)
    return skewed[:, :, :key_rows]


def attend(queries, keys_all, values_all, query_pos, key_pos, query_doc, key_doc, bias_table):
    query_rows = queries.shape[0]
    key_rows = keys_all.shape[0]
    reach_rows = key_rows - query_rows
    scores = jnp.einsum(
        "qhe,khe->hqk", queries, keys_all, preferred_element_type=jnp.float32
    ) * HEAD_DIM ** (-0.5)
    scores = scores + banded_bias(bias_table, query_rows, key_rows, reach_rows)
    query_seg = query_pos // SEG
    key_seg = key_pos // SEG
    allowed = (
        (key_pos[None, :] >= 0)
        & (key_seg[None, :] <= query_seg[:, None])
        & (key_seg[None, :] >= query_seg[:, None] - LEFT)
        & (key_doc[None, :] == query_doc[:, None])
    )
    scores = jnp.where(allowed[None], scores, -1e30)
    peak = jnp.max(scores, axis=-1, keepdims=True)
    raised = jnp.exp(scores - peak)
    weights_bf = (raised / jnp.sum(raised, axis=-1, keepdims=True)).astype(jnp.bfloat16)
    return jnp.einsum(
        "hqk,khe->qhe", weights_bf, values_all, preferred_element_type=jnp.float32
    ).astype(jnp.bfloat16)


def body(tokens, documents, norm_gain, w_query, w_key, w_value, w_out, rel_bias):
    local_rows = tokens.shape[0]
    reach_rows = LEFT * SEG
    width_local = w_query.shape[2]
    heads_local = width_local // HEAD_DIM
    offset = lax.axis_index("sp") * local_rows
    query_pos = offset + jnp.arange(local_rows, dtype=jnp.int32)
    key_pos = offset - reach_rows + jnp.arange(reach_rows + local_rows, dtype=jnp.int32)
    widened = tokens.astype(jnp.float32)
    normed = (
        widened
        * lax.rsqrt(jnp.mean(widened * widened, axis=-1, keepdims=True) + EPS)
        * norm_gain[0]
    ).astype(jnp.bfloat16)
    query_sum = jnp.dot(
        normed,
        lax.all_gather(w_query[0], "sp", axis=0, tiled=True),
        preferred_element_type=jnp.float32,
    )
    key_sum = jnp.dot(
        normed,
        lax.all_gather(w_key[0], "sp", axis=0, tiled=True),
        preferred_element_type=jnp.float32,
    )
    value_sum = jnp.dot(
        normed,
        lax.all_gather(w_value[0], "sp", axis=0, tiled=True),
        preferred_element_type=jnp.float32,
    )
    queries = query_sum.astype(jnp.bfloat16)
    keys_own = key_sum.astype(jnp.bfloat16)
    values_own = value_sum.astype(jnp.bfloat16)
    prior_keys, prior_values, prior_docs = passed_along((keys_own, values_own, documents), "sp", 1)
    keys_all = jnp.concatenate([prior_keys, keys_own], axis=0)
    values_all = jnp.concatenate([prior_values, values_own], axis=0)
    key_doc = jnp.concatenate([prior_docs, documents], axis=0)
    attended = attend(
        queries.reshape(local_rows, heads_local, HEAD_DIM),
        keys_all.reshape(reach_rows + local_rows, heads_local, HEAD_DIM),
        values_all.reshape(reach_rows + local_rows, heads_local, HEAD_DIM),
        query_pos,
        key_pos,
        documents,
        key_doc,
        rel_bias[0],
    ).reshape(local_rows, width_local)
    all_heads = lax.all_gather(attended, "tp", axis=1, tiled=True)
    return (
        widened
        + jnp.dot(
            all_heads,
            lax.all_gather(w_out[0], "sp", axis=1, tiled=True),
            preferred_element_type=jnp.float32,
        )
    ).astype(jnp.bfloat16)


MESH = pl.DeviceIdType.MESH
TOK, OUT = range(2)
UP, DOWN, ACROSS = range(3)
W0, W1, A0, A1 = range(4)
NEG = -1e30


def plane_of(t):
    c = t % 2
    return 3 * c + (t // 2) * (1 - 2 * c)


def part_for(z):
    return 2 * (((z + 1) // 2) % 2) + z // 2


def layer_kernel(
    n_sp, n_tp, doc_in, gain_in, table_in, x_in, wk_in, wv_in, wq_in, wo_in, out_ref,
    w_own, w_relay, w_all, wo_all, tok, aid, wo_aid, resid, normed, gain, table, bias, q_buf, kv_all, docs_all, mask,
    att_own, att_relay, att_all,
    own_sem, loc_sem, out_sem, tok_sem, aid_sem, aid_send, wo_aid_sem, wo_aid_send, res_sem, small_sem, line_send, line_recv, hop_send, relay_recv, rep_send, rep_recv,
    cast_send, cast_recv, across_recv, halo_send, halo_recv, tp_send, tp_recv,
):
    rows, width = tok.shape[1:]
    depth, cols = wk_in.shape
    half_cols = cols // 2
    lanes = 2 * HEAD_DIM
    pairs = half_cols // lanes
    q_rows, span = 2 * SEG, (LEFT + 2) * SEG
    chunk = width // n_tp
    nz = n_sp // 2
    pieces = 2 * n_tp
    aids = n_tp
    piece = rows // pieces
    s = lax.axis_index("sp")
    t = lax.axis_index("tp")
    z, x = s // 2, s % 2
    mate = s + 1 - 2 * x
    ty, tc = t // 2, t % 2
    t_core = t + 1 - 2 * tc
    t_y = (1 - ty) * 2 + tc
    t_far = (1 - ty) * 2 + 1 - tc
    home, home_y = plane_of(t), plane_of(t_y)
    first_entry, second_entry = z == home, z == home_y
    entry = first_entry | second_entry
    gap = z - home
    is_first = 1 - (gap * gap + n_sp) // (n_sp + 1)
    x_mine = x * is_first + (1 - x) * (1 - is_first)
    own_in = (wk_in, wv_in, wq_in)
    has_up, has_down = z < nz - 1, z > 0

    def at_multiple(start, size, step):
        return pl.ds(pl.multiple_of(start, step), size)

    def weight_cols(which, p):
        return at_multiple(which * half_cols + p * lanes, lanes, lanes)

    def kind_cols(kind):
        return pl.ds(kind * lanes, lanes)

    def own_copy(i, p, kind):
        which = x if i == 0 else 1 - x
        return pltpu.make_async_copy(
            own_in[kind].at[:, weight_cols(which, p)], w_own.at[i, p, :, kind_cols(kind)], own_sem.at[i, p]
        )

    def local_copy(p, kind):
        return pltpu.make_async_copy(
            own_in[kind].at[:, weight_cols(x, p)],
            w_all.at[p, at_multiple(s * depth, depth, depth), kind_cols(kind)], loc_sem.at[p],
        )

    tok_copy = pltpu.make_async_copy(x_in, tok.at[x], tok_sem)

    def out_copy(r):
        return pltpu.make_async_copy(wo_in.at[pl.ds(r * cols, cols), :], wo_all.at[2 * r + x], out_sem.at[r])

    doc_copy = pltpu.make_async_copy(doc_in, docs_all.at[:, at_multiple((1 + x) * rows, rows, rows)], small_sem.at[0])
    gain_copy = pltpu.make_async_copy(gain_in, gain, small_sem.at[1])
    table_copy = pltpu.make_async_copy(table_in, table, small_sem.at[2])
    resid_copy = pltpu.make_async_copy(x_in.at[:, at_multiple(home_y * chunk, chunk, chunk)], resid, res_sem)

    gain_copy.start()

    @pl.when(first_entry)
    def _():
        doc_copy.start()
        tok_copy.start()
        table_copy.start()

    for p in range(pairs):
        for i in (1, 0):
            for kind in range(3):
                own_copy(i, p, kind).start()

    @pl.when(first_entry)
    def _():
        for p in range(pairs):
            for kind in range(3):
                local_copy(p, kind).start()

    outer = (z == 0) | (z == nz - 1)
    inner = jnp.logical_not(outer)
    lower = z < nz // 2
    aid_copy = pltpu.make_async_copy(x_in.at[pl.ds(rows - 4 * piece, 4 * piece), :], aid, aid_sem)

    def wo_aid_copy(r):
        return pltpu.make_async_copy(wo_in.at[pl.ds(r * cols, cols), :], wo_aid.at[r - 1], wo_aid_sem.at[r - 1])

    aide = inner & (z == plane_of(t_far))

    @pl.when(aide)
    def _():
        for r in range(1, n_tp):
            wo_aid_copy(r).start()

    @pl.when(second_entry)
    def _():
        pl.when(inner)(lambda: aid_copy.start())

        for r in range(n_tp):
            out_copy(r).start()

    resid_copy.start()

    def remote(src, dst, send, recv, **where):
        return pltpu.make_async_remote_copy(
            src_ref=src, dst_ref=dst, send_sem=send, recv_sem=recv, device_id=where, device_id_type=MESH
        )

    def slot(ch, block):
        if ch < A0:
            return w_all.at[ch - W0, at_multiple(block * depth, depth, depth), :]
        return att_all.at[
            part_for(block // 2), pl.ds((ch - A0) * q_rows, q_rows), at_multiple((block % 2) * half_cols, half_cols, half_cols)
        ]

    def own_ref(ch, i):
        return w_own.at[i, ch - W0] if ch < A0 else att_own.at[ch - A0, x if i == 0 else 1 - x]

    def relay_ref(ch):
        return w_relay.at[ch - W0] if ch < A0 else att_relay.at[ch - A0]

    def direct(ch):
        return remote(own_ref(ch, 0), slot(ch, s), hop_send.at[ch, 0], rep_recv.at[ch, s], sp=2 * home + x)

    def cross_in(ch):
        return remote(own_ref(ch, 1), slot(ch, s), hop_send.at[ch, 1], rep_recv.at[ch, s], sp=mate, tp=t_y)

    def cross_relay(ch):
        return remote(own_ref(ch, 1), relay_ref(ch), hop_send.at[ch, 1], relay_recv.at[ch], sp=mate, tp=t_y)

    def relay(ch):
        return remote(relay_ref(ch), slot(ch, mate), hop_send.at[ch, 2], rep_recv.at[ch, mate], sp=2 * home_y + x)

    def to_y(ch, block):
        return remote(slot(ch, block), slot(ch, block), rep_send.at[ch, 0], rep_recv.at[ch, block], tp=t_y)

    def to_core(ch, block):
        return remote(slot(ch, block), slot(ch, block), rep_send.at[ch, 1], rep_recv.at[ch, block], tp=t_core)

    def send_cross(ch):
        pl.when(first_entry)(lambda: cross_in(ch).start())
        pl.when(jnp.logical_not(first_entry))(lambda: cross_relay(ch).start())

    def send_direct(ch):
        pl.when(jnp.logical_not(first_entry))(lambda: direct(ch).start())

    def send_relay(ch):
        @pl.when(jnp.logical_not(second_entry))
        def _():
            cross_relay(ch).wait_recv()
            relay(ch).start()

    planes = [0]
    for d in range(1, nz):
        planes += [-d, d]

    def valid(off):
        return (z + off >= 0) & (z + off < nz)

    def mine(ch, off):
        @pl.when(entry & valid(off))
        def _():
            block = 2 * (z + off) + x_mine
            if off == 0:
                pl.when(jnp.logical_not(first_entry))(lambda: to_y(ch, block).wait_recv())
                if ch < A0:
                    @pl.when(first_entry)
                    def _():
                        wide = wk_in.at[:, pl.ds(0, 3 * lanes)]
                        pltpu.make_async_copy(wide, slot(ch, s), loc_sem.at[ch - W0]).wait()
            else:
                to_y(ch, block).wait_recv()
            to_y(ch, block).start()
            to_core(ch, block).start()

    def theirs(ch, off):
        @pl.when(valid(off))
        def _():
            @pl.when(entry)
            def _():
                block = 2 * (z + off) + 1 - x_mine
                to_y(ch, block).wait_recv()
                to_core(ch, block).start()

            @pl.when(jnp.logical_not(entry))
            def _():
                for i in range(2):
                    to_core(ch, 2 * (z + off) + i).wait_recv()

    def spread(ch, first, last):
        for i in range(first, last + 1):
            if i < len(planes):
                mine(ch, planes[i])
            if i > 0:
                theirs(ch, planes[i - 1])

    def drain(ch):
        pl.when(jnp.logical_not(first_entry))(lambda: direct(ch).wait_send())
        cross_relay(ch).wait_send()
        pl.when(jnp.logical_not(second_entry))(lambda: relay(ch).wait_send())

        @pl.when(entry)
        def _():
            if ch < A0:
                some, every = w_all.at[ch - W0, pl.ds(0, nz * depth), :], w_all.at[ch - W0]
            else:
                some, every = att_all.at[0], att_all.at[pl.ds(0, 2)]
            remote(some, some, rep_send.at[ch, 0], rep_recv.at[ch, 0], tp=t_y).wait_send()
            remote(every, every, rep_send.at[ch, 1], rep_recv.at[ch, 0], tp=t_core).wait_send()

    def cast_ref(kind, which, r):
        if kind == OUT:
            return wo_all.at[2 * r + which]
        if r == pieces:
            return docs_all.at[:, at_multiple((1 + which) * rows, rows, rows)]
        return tok.at[which, pl.ds(r * piece, piece), :]

    def group_of(kind, r):
        if kind == OUT:
            return 3 if r == 0 else 4
        return 2 if r == pieces else int(r >= pieces - aids)

    def line_in(kind, r):
        return cast_recv.at[r if kind == TOK else pieces + 1 + r]

    def move(kind, way, r):
        ref = cast_ref(kind, x, r)
        arrive = across_recv.at[(0, 0, 1, 2, 2)[group_of(kind, r)]] if way == ACROSS else line_in(kind, r)
        return remote(ref, ref, cast_send.at[group_of(kind, r), way], arrive, sp=(s + 2, s - 2, mate)[way])

    aid_rows = aids * piece
    whole = (
        tok.at[0, pl.ds(0, rows - aid_rows), :], tok.at[0, pl.ds(0, aid_rows), :], docs_all.at[:, pl.ds(0, rows)],
        wo_all.at[0], wo_all.at[pl.ds(0, n_tp - 1)],
    )

    def across_all(i):
        ref = (tok.at[1 - x], docs_all.at[:, at_multiple((2 - x) * rows, rows, rows)], wo_all.at[pl.ds(0, n_tp)])[i]
        return remote(ref, ref, cast_send.at[0, ACROSS], across_recv.at[i], sp=mate)

    centers = (home, home_y)

    def aided(kind, r):
        return pieces - aids <= r < pieces if kind == TOK else r > 0

    def goes(kind, way, r):
        ok = (z >= centers[kind]) & has_up if way == UP else (z <= centers[kind]) & has_down
        if aided(kind, r):
            near = jnp.logical_not(lower) if way == UP else lower
            ok = ok & jnp.logical_not((z == centers[kind]) & inner & near)
        return ok

    def aid_move(i):
        r = pieces - aids + i
        return remote(
            aid.at[pl.ds(i * piece, piece), :], cast_ref(TOK, x, r), aid_send, line_in(TOK, r),
            sp=s + 2 - 4 * (1 - z // (nz // 2)), tp=t_y,
        )

    def wo_aid_move(r):
        return remote(
            wo_aid.at[r - 1], cast_ref(OUT, x, r), wo_aid_send.at[r - 1], line_in(OUT, r),
            sp=s + 2 - 4 * (1 - z // (nz // 2)), tp=t_core,
        )

    def cast_along(kind, r):
        for way in (UP, DOWN):
            pl.when(goes(kind, way, r))(lambda: move(kind, way, r).start())

    def cast_send_on(kind, r):
        cast_along(kind, r)
        move(kind, ACROSS, r).start()

    def cast_source(kind, r):
        if r == pieces and kind == TOK:
            doc_copy.wait()
            cast_send_on(kind, r)
            return
        if kind == OUT:
            out_copy(r).wait()
        elif r == 0:
            tok_copy.wait()
        cast_send_on(kind, r)

    def cast_forward(kind, r):
        @pl.when(z != centers[kind])
        def _():
            move(kind, UP, r).wait_recv()
            cast_send_on(kind, r)

    def cast_drain():
        for g, (kind, r) in enumerate(((TOK, 0), (TOK, pieces - 1), (TOK, pieces), (OUT, 0), (OUT, 1))):
            def done(way):
                remote(whole[g], whole[g], cast_send.at[g, way], line_in(kind, r), sp=mate).wait_send()

            for way in (UP, DOWN):
                pl.when(goes(kind, way, r))(lambda: done(way))
            done(ACROSS)

    line_targets = (t_core, t_y, t_far)

    def line_copy(i):
        return remote(table, table, line_send.at[i], line_recv, tp=line_targets[i])

    has_next, has_prev = home < nz - 1, home > 0

    def halo(i):
        if i == pairs:
            src, dst = docs_all.at[:, pl.ds(2 * rows, rows)], docs_all.at[:, pl.ds(0, rows)]
        else:
            src, dst = kv_all.at[i, pl.ds(2 * rows, rows), :], kv_all.at[i, pl.ds(0, rows), :]
        return remote(src, dst, halo_send.at[i], halo_recv.at[i], tp=part_for((home + 1) % nz))

    barrier = pltpu.get_barrier_semaphore()
    for d in range(1, nz):
        pl.semaphore_signal(
            barrier, inc=1, device_id={"sp": lax.rem(s + 2 * d, n_sp)}, device_id_type=MESH
        )
    for peer in (t_core, t_y, t_far):
        pl.semaphore_signal(barrier, inc=1, device_id={"tp": peer}, device_id_type=MESH)
    for peer in (t, t_y):
        pl.semaphore_signal(barrier, inc=1, device_id={"sp": mate, "tp": peer}, device_id_type=MESH)
    pl.semaphore_signal(
        barrier, inc=1, device_id={"sp": s + 2 - 4 * (z % 2), "tp": t_y}, device_id_type=MESH
    )
    pl.semaphore_signal(
        barrier, inc=1, device_id={"sp": s + 2 - 4 * (z % 2), "tp": t_core}, device_id_type=MESH
    )
    pl.semaphore_wait(barrier, nz + 6)

    for p in range(pairs):
        for i in (1, 0):
            wide = wk_in.at[:, pl.ds(0, 3 * lanes)]
            pltpu.make_async_copy(wide, w_own.at[i, p], own_sem.at[i, p]).wait()
            (send_direct, send_cross)[i](W0 + p)

    @pl.when(first_entry)
    def _():
        for r in (pieces,) + tuple(range(pieces)):
            if r in (2, 3):
                pl.when((z <= home) & has_up & (outer | lower))(lambda: move(TOK, UP, r).start())
                pl.when((z >= home) & has_down & (outer | jnp.logical_not(lower)))(lambda: move(TOK, DOWN, r).start())
                move(TOK, ACROSS, r).start()
            else:
                cast_source(TOK, r)
        table_copy.wait()
        for i in range(3):
            line_copy(i).start()

    def out_along(r):
        out_copy(r).wait()
        cast_along(OUT, r)

    def out_near(r):
        pl.when(goes(OUT, UP, r) & jnp.logical_not(lower))(lambda: move(OUT, UP, r).start())
        pl.when(goes(OUT, DOWN, r) & lower)(lambda: move(OUT, DOWN, r).start())

    def out_far(r):
        pl.when(goes(OUT, UP, r) & lower)(lambda: move(OUT, UP, r).start())
        pl.when(goes(OUT, DOWN, r) & jnp.logical_not(lower))(lambda: move(OUT, DOWN, r).start())

    def out_across(r):
        move(OUT, ACROSS, r).start()

    def out_pass(r):
        @pl.when(z != home_y)
        def _():
            move(OUT, UP, r).wait_recv()
            cast_along(OUT, r)

    @pl.when(second_entry)
    def _():
        @pl.when(inner)
        def _():
            aid_copy.wait()
            for i in range(aids):
                aid_move(i).start()

        @pl.when(outer)
        def _():
            for r in range(n_tp):
                out_along(r)

    @pl.when(has_prev == False)
    def _():
        docs_all[:, pl.ds(0, rows)] = jnp.full((1, rows), -1, jnp.int32)
        for p in range(pairs):
            kv_all[p, pl.ds(0, rows), :] = jnp.zeros((rows, 2 * lanes), jnp.bfloat16)

    def around(d):
        return (0,) if d == 0 else (-d, d)

    def pass_mine(ch, d):
        for off in around(d):
            mine(ch, off)

    def pass_theirs(ch, d):
        for off in around(d):
            theirs(ch, off)

    @pl.when(first_entry)
    def _():
        pass_mine(W0, 0)
        pass_mine(W1, 0)
        send_relay(W0)
        send_relay(W1)

        @pl.when(inner)
        def _():
            for r in (2, 3):
                pl.when(lower)(lambda: move(TOK, DOWN, r).start())
                pl.when(jnp.logical_not(lower))(lambda: move(TOK, UP, r).start())

        for ch in (W0, W1):
            for d in range(1, nz):
                pass_mine(ch, d)

        @pl.when(inner)
        def _():
            for r in range(n_tp):
                out_pass(r)
                if r < 2:
                    out_across(r)

        @pl.when(outer)
        def _():
            out_pass(0)
            out_across(0)

        for ch in (W0, W1):
            for d in range(nz):
                pass_theirs(ch, d)

    @pl.when(second_entry)
    def _():
        pass_mine(W0, 0)
        cast_forward(TOK, pieces)
        for r in range(0, 2):
            cast_forward(TOK, r)

        @pl.when(inner)
        def _():
            out_copy(0).wait()
            out_near(0)

        out_across(0)
        pass_mine(W1, 0)
        for r in range(2, 4):
            cast_forward(TOK, r)
        pl.when(inner)(lambda: out_copy(1).wait())
        out_across(1)
        pass_mine(W0, 1)
        pass_mine(W1, 1)
        for r in range(4, 6):
            cast_forward(TOK, r)
        pass_mine(W0, 2)
        pass_mine(W1, 2)
        for r in range(6, 8):
            cast_forward(TOK, r)
        pass_mine(W0, 3)
        pass_mine(W1, 3)

        @pl.when(inner)
        def _():
            for r in range(n_tp):
                if r >= 2:
                    out_copy(r).wait()
                out_far(r)

        for ch in (W0, W1):
            for d in range(nz):
                pass_theirs(ch, d)

    @pl.when(jnp.logical_not(entry))
    def _():
        send_relay(W0)
        send_relay(W1)
        for r in (pieces,) + tuple(range(pieces)):
            cast_forward(TOK, r)

        @pl.when(aide)
        def _():
            for r in range(1, n_tp):
                wo_aid_copy(r).wait()
                wo_aid_move(r).start()

        pl.when(inner)(lambda: out_pass(0))
        for ch in (W0, W1):
            for d in range(nz):
                pass_theirs(ch, d)


    gain_copy.wait()

    def normalize(which):
        wide = tok[which].astype(jnp.float32)
        normed[at_multiple(which * rows, rows, rows), :] = (
            wide * lax.rsqrt(jnp.mean(wide * wide, axis=-1, keepdims=True) + EPS) * gain[...]
        ).astype(jnp.bfloat16)

    normalize(x)

    heads = half_cols // HEAD_DIM
    blocks = 2 * rows // q_rows

    pl.when(jnp.logical_not(first_entry))(lambda: line_copy(0).wait_recv())
    q_seg = lax.broadcasted_iota(jnp.int32, (q_rows, span), 0) // SEG
    k_seg = lax.broadcasted_iota(jnp.int32, (q_rows, span), 1) // SEG
    near = (k_seg >= q_seg) & (k_seg <= q_seg + LEFT)
    length = table.shape[1]
    line_len = (LEFT + 4) * SEG
    entry_of = lax.broadcasted_iota(jnp.int32, (length, line_len), 0)
    back = LEFT * SEG - lax.broadcasted_iota(jnp.int32, (length, line_len), 1)
    back = jnp.where(back < -REL_CLIP, REL_CLIP, jnp.minimum(back, REL_CLIP))
    pick = (entry_of == back + REL_CLIP).astype(jnp.float32)
    lines = jnp.dot(table[...], pick, precision=lax.Precision.HIGHEST, preferred_element_type=jnp.float32)
    lines = jnp.where(x == 0, lines[:heads], lines[heads:])
    for h in range(heads):
        line = jnp.broadcast_to(lines[h : h + 1, :], (q_rows, line_len))
        skew = pltpu.roll(line, 0, 1, stride=1, stride_axis=0)
        bias[h] = jnp.where(near, skew[:, :span], NEG)

    def project(which):
        own = at_multiple(which * rows, rows, rows)
        for p in range(pairs):
            made = jnp.dot(normed[own, :], w_all[p], preferred_element_type=jnp.float32).astype(jnp.bfloat16)
            kv_all[p, at_multiple((1 + which) * rows, rows, rows), :] = made[:, : 2 * lanes]
            q_buf[p, own, :] = (made[:, 2 * lanes :].astype(jnp.float32) * HEAD_DIM ** (-0.5)).astype(jnp.bfloat16)

    def send_halo():
        for p in range(pairs):
            halo(p).start()

    project(x)
    pl.when(has_next & (x == 1))(send_halo)
    middle = jnp.logical_not(entry) & inner

    pl.when(middle)(lambda: out_pass(1))
    for i in range(2):
        across_all(i).wait_recv()
    pl.when(has_next)(lambda: halo(pairs).start())
    normalize(1 - x)
    late = jnp.logical_not(second_entry) & outer
    project(1 - x)
    pl.when(has_next & (x == 0))(send_halo)

    low = lax.broadcasted_iota(jnp.int32, (q_rows, lanes), 1) < HEAD_DIM
    eye = lax.broadcasted_iota(jnp.int32, (q_rows, q_rows), 0) == lax.broadcasted_iota(jnp.int32, (q_rows, q_rows), 1)

    def make_mask(j):
        q_docs = docs_all[pl.ds(0, 1), pl.ds(rows + j * q_rows, q_rows)].astype(jnp.float32)
        k_docs = docs_all[pl.ds(0, 1), pl.ds(j * q_rows, span)].astype(jnp.float32)
        column = jnp.sum(jnp.where(eye, jnp.broadcast_to(q_docs, (q_rows, q_rows)), 0.0), axis=1, keepdims=True)
        mask[j] = jnp.where(column == k_docs, 0.0, NEG)

    def attend_rows(g):
        keys, queries = pl.ds(g * q_rows, span), pl.ds(g * q_rows, q_rows)
        found = []
        for p in range(pairs):
            q_pair = q_buf[p, queries, :]
            k_pair = kv_all[p, keys, pl.ds(0, lanes)]
            v_pair = kv_all[p, keys, pl.ds(lanes, lanes)]
            both = []
            for half in range(2):
                on = low if half == 0 else jnp.logical_not(low)
                q_one = jnp.where(on, q_pair, jnp.zeros_like(q_pair))
                score = lax.dot_general(q_one, k_pair, (((1,), (1,)), ((), ())), preferred_element_type=jnp.float32)
                score = score + bias[2 * p + half] + mask[g]
                raised = jnp.exp(score - jnp.max(score, axis=-1, keepdims=True))
                total = jnp.sum(raised, axis=-1, keepdims=True)
                both.append(jnp.dot(raised.astype(jnp.bfloat16), v_pair, preferred_element_type=jnp.float32) / total)
            found.append(jnp.where(low, both[0], both[1]).astype(jnp.bfloat16))
        return jnp.concatenate(found, axis=1)

    per = blocks // 2

    def attend_step(j, which):
        found = attend_rows(which * per + j)
        att_own[j, which] = found

        @pl.when(first_entry & (x == which))
        def _():
            att_all[t, pl.ds(j * q_rows, q_rows), at_multiple(x * half_cols, half_cols, half_cols)] = found

        pl.when(x == which)(lambda: send_direct(A0 + j))
        pl.when(x != which)(lambda: send_cross(A0 + j))

    for g in range(per, blocks):
        make_mask(g)
    attend_step(0, 1)
    pl.when(middle)(lambda: out_pass(2))
    attend_step(1, 1)
    pl.when(middle)(lambda: out_pass(3))

    @pl.when(has_prev)
    def _():
        for i in (pairs,) + tuple(range(pairs)):
            halo(i).wait_recv()

    for g in range(per):
        make_mask(g)
    attend_step(0, 0)
    attend_step(1, 0)
    third = jnp.logical_not(entry)
    pl.when(third & outer)(lambda: out_pass(0))
    pl.when(third)(lambda: out_across(0))
    pl.when(first_entry & outer)(lambda: out_pass(1))
    pl.when(first_entry & outer)(lambda: out_across(1))
    send_relay(A0)
    send_relay(A1)
    pl.when(third & outer)(lambda: out_pass(1))
    pl.when(third)(lambda: out_across(1))
    swift = jnp.logical_not(late)

    @pl.when(swift)
    def _():
        out_across(2)
        out_across(3)

    for d in range(nz):
        for ch in (A0, A1):
            pass_mine(ch, d)

    @pl.when(late)
    def _():
        for r in (2, 3):
            out_pass(r)
            out_across(r)

    half_chunk = chunk // 2

    def result(which, j, i):
        cut = at_multiple(which * chunk + i * half_chunk, half_chunk, half_chunk)
        return out_ref.at[pl.ds(j * q_rows, q_rows), cut]

    def tp_move(way, j, i):
        which, target = ((home_y, t_y), (home_y, t_core), (home, t_core))[way]
        ref = result(which, j, i)
        return remote(ref, ref, tp_send.at[way], tp_recv.at[way, j, i], tp=target)

    def out_project(j, i):
        part = pl.ds(j * q_rows, q_rows)
        made = jnp.zeros((q_rows, half_chunk), jnp.float32)
        for r in range(n_tp):
            made = made + jnp.dot(att_all[r, part, :], wo_all[2 * r + i], preferred_element_type=jnp.float32)
        rest = resid[part, at_multiple(i * half_chunk, half_chunk, half_chunk)].astype(jnp.float32)
        result(home_y, j, i)[...] = (rest + made).astype(jnp.bfloat16)
        tp_move(0, j, i).start()
        tp_move(1, j, i).start()

    resid_copy.wait()
    for j in range(per):
        for d in range(nz):
            pass_theirs(A0 + j, d)
        out_project(j, x)
    across_all(2).wait_recv()
    for j in range(per):
        out_project(j, 1 - x)
    quarters = [(j, i) for i in (x, 1 - x) for j in range(per)]
    for q in quarters:
        tp_move(0, *q).wait_recv()
        tp_move(2, *q).start()
    for q in quarters:
        tp_move(1, *q).wait_recv()
        tp_move(2, *q).wait_recv()

    for ch in range(4):
        drain(ch)
    cast_drain()

    @pl.when(second_entry & inner)
    def _():
        remote(aid, whole[1], aid_send, line_in(TOK, 0), tp=t_y).wait_send()

    @pl.when(aide)
    def _():
        for r in range(1, n_tp):
            wo_aid_move(r).wait_send()


    @pl.when(first_entry)
    def _():
        for i in range(3):
            line_copy(i).wait_send()

    @pl.when(has_next)
    def _():
        for i in range(pairs + 1):
            halo(i).wait_send()
    for way in range(3):
        ref = out_ref.at[:, pl.ds(0, chunk)]
        remote(ref, ref, tp_send.at[way], tp_recv.at[way, 0, 0], tp=t_y).wait_send()


def body_one(n_sp, n_tp, tokens, documents, norm_gain, w_query, w_key, w_value, w_out, rel_bias):
    rows, width = tokens.shape
    depth, cols = w_query.shape[1:]
    heads = cols // HEAD_DIM
    out_cols = w_out.shape[2]
    chunk = width // n_tp
    lanes = 2 * HEAD_DIM
    pairs = cols // 2 // lanes
    table = rel_bias[0]
    bf, f32 = jnp.bfloat16, jnp.float32
    hbm = pl.BlockSpec(memory_space=pl.ANY)
    dma = pltpu.SemaphoreType.DMA
    q_rows, span = 2 * SEG, (LEFT + 2) * SEG
    return pl.pallas_call(
        functools.partial(layer_kernel, n_sp, n_tp),
        out_shape=pltpu.VMEM((rows, width), bf),
        in_specs=[hbm] * 8,
        out_specs=pl.BlockSpec(memory_space=pltpu.VMEM),
        scratch_shapes=[
            pltpu.VMEM((2, pairs, depth, 3 * lanes), bf),
            pltpu.VMEM((pairs, depth, 3 * lanes), bf),
            pltpu.VMEM((pairs, n_sp * depth, 3 * lanes), bf),
            pltpu.VMEM((n_sp, cols, out_cols), bf),
            pltpu.VMEM((2, rows, width), bf),
            pltpu.VMEM((4 * rows // (2 * n_tp), width), bf),
            pltpu.VMEM((n_tp - 1, cols, out_cols), bf),
            pltpu.VMEM((rows, chunk), bf),
            pltpu.VMEM((2 * rows, width), bf),
            pltpu.VMEM((1, width), f32),
            pltpu.VMEM(table.shape, f32),
            pltpu.VMEM((heads // 2, q_rows, span), f32),
            pltpu.VMEM((pairs, 2 * rows, lanes), bf),
            pltpu.VMEM((pairs, 3 * rows, 2 * lanes), bf),
            pltpu.VMEM((1, 3 * rows), jnp.int32),
            pltpu.VMEM((2 * rows // q_rows, q_rows, span), f32),
            pltpu.VMEM((rows // q_rows, 2, q_rows, cols // 2), bf),
            pltpu.VMEM((rows // q_rows, q_rows, cols // 2), bf),
            pltpu.VMEM((n_tp, rows, cols), bf),
            dma((2, pairs)),
            dma((pairs,)),
            dma((n_tp,)),
            dma(()),
            dma(()),
            dma(()),
            dma((n_tp - 1,)),
            dma((n_tp - 1,)),
            dma(()),
            dma((3,)),
            dma((3,)),
            dma(()),
            dma((4, 3)),
            dma((4,)),
            dma((4, 2)),
            dma((4, n_sp)),
            dma((5, 3)),
            dma((3 * n_tp + 1,)),
            dma((3,)),
            dma((pairs + 1,)),
            dma((pairs + 1,)),
            dma((3,)),
            dma((3, rows // q_rows, 2)),
        ],
        compiler_params=pltpu.CompilerParams(
            collective_id=0, has_side_effects=True, vmem_limit_bytes=60 * 1024 * 1024
        ),
    )(documents[None, :], norm_gain, table, tokens, w_key[0], w_value[0], w_query[0], w_out[0])


def fits_one(mesh):
    return mesh.shape["tp"] == 4 and mesh.shape["sp"] == 2 * mesh.shape["tp"]


def solution(mesh):
    n_sp, n_tp = mesh.shape["sp"], mesh.shape["tp"]
    run = functools.partial(body_one, n_sp, n_tp) if fits_one(mesh) else body
    in_specs = (
        P("sp", None),
        P("sp"),
        P(),
        P(None, "sp", "tp"),
        P(None, "sp", "tp"),
        P(None, "sp", "tp"),
        P(None, None, "sp"),
        P(None, "tp", None),
    )
    out_specs = P("sp", None)
    return jax.shard_map(run, mesh=mesh, in_specs=in_specs, out_specs=out_specs, check_vma=False)
```
